256 devices in a mesh: ep: 64 (over z, x, core), tp: 4 (over y).
Axes of the slice: x: 4, y: 4, z: 8, core: 2. Of those that a mesh axis runs over, the one named last changes fastest.
Arguments:
- conv_input: bfloat16 [32768, 2048], P(('ep', 'tp')), may hold values from -6 to 6
- conv_kernel: float32 [31, 2048], replicated, may hold values from -1 to 1
- conv_gain: float32 [2048], replicated, may hold values from 0.1 to 1.9
- out_weight: bfloat16 [2048, 2048], P(None, 'tp'), may hold values from -0.125 to 0.125
- moe_input: bfloat16 [32768, 2048], P(('ep', 'tp')), may hold values from -6 to 6
- moe_gain: float32 [2048], replicated, may hold values from 0.1 to 1.9
- expert_gate: bfloat16 [64, 2048, 2048], P('ep', None, 'tp'), may hold values from -0.125 to 0.125
- expert_up: bfloat16 [64, 2048, 2048], P('ep', None, 'tp'), may hold values from -0.125 to 0.125
- expert_down: bfloat16 [64, 2048, 2048], P('ep', 'tp'), may hold values from -0.125 to 0.125
- shared_gate: bfloat16 [2048, 128], replicated, may hold values from -0.125 to 0.125
- shared_up: bfloat16 [2048, 128], replicated, may hold values from -0.125 to 0.125
- shared_down: bfloat16 [128, 2048], replicated, may hold values from -0.5 to 0.5
- expert_index: int32 [32768, 2], P('ep'), may hold values from 0 to 63, all different within a row; in each aligned block of 128 rows (0 to 127, 128 to 255, ...) at most 6 rows name the same one
- routing_weight: float32 [32768, 2], P(('ep', 'tp')), may hold values from 0.25 to 1.5
Outputs:
- conv_out: bfloat16 [32768, 2048], P('ep', 'tp')
- moe_out: bfloat16 [32768, 2048], P(('ep', 'tp'))
The draws below stay inside these ranges and needn't reach their ends.
Inputs may be any that keep to these rules, and one draw needn't show every extreme that they name: `expert_index`: each row names 2 different experts. In each aligned block of 128 rows no expert is named by more than 6 of the rows, and in some blocks one expert is named by exactly 6 rows.
All inputs are finite; a program needn't handle non-finite values.
Results may differ from the reference program's by a relative error of at most 0.009.
Values may be sent and summed in bfloat16 or wider, within the bound.
A program may use at most 128 MiB of HBM per device.

```python
import math
import jax
import jax.numpy as jnp
import numpy as np
from jax import lax

D = 2048
FF = 2048
SHARED_FF = 128
TOPK = 2
KERNEL = 31
TOK_DEV_B = 128
TOKENS_A = 32768
TOKENS_B = 32768
EXPERTS = 64
SLOTS = 6
N_TP = 4


def level_of(key, dims, cuts, smallest, largest):
    def one(axis_at, blocks):
        heights = jax.random.uniform(jax.random.fold_in(jax.random.fold_in(key, 6), axis_at), (blocks,), jnp.float32, smallest / len(cuts), largest / len(cuts))
        return jnp.repeat(jnp.exp(heights), dims[axis_at] // blocks).reshape((-1,) + (1,) * (len(dims) - axis_at - 1))

    level = one(*cuts[0])
    for cut in cuts[1:]:
        level = level * one(*cut)
    return level


def shared_out(key, own, number, rows, number_of, top, limit, slope):
    sequence = jax.random.permutation(key, number_of)
    crowded, common = shares(number_of, rows * top, limit, slope, True), shares(number_of, rows * top, limit, slope, False)
    places = jnp.arange(number_of)

    def named(sizes, rotation):
        used = int((sizes > 0).sum())
        fixed = max(1, used // 4)
        moved = fixed + (places - fixed + rotation * (used - fixed)) % max(1, number_of - fixed)
        return jnp.zeros((number_of,), jnp.int32).at[sequence[jnp.where(places < fixed, places, moved)]].set(jnp.asarray(sizes, jnp.int32))

    sizes = jnp.where(number % 4 == 0, named(crowded, number // 4), named(common, number - number // 4 - 1))
    mixed = jax.random.permutation(jax.random.fold_in(own, 3), number_of)
    donor, receiver = mixed[0:number_of // 2 * 2:2], mixed[1:number_of // 2 * 2:2]
    slack = jnp.minimum(sizes[donor] - 1, limit - sizes[receiver]) // 2
    slack = jnp.where((donor == sequence[0]) | (receiver == sequence[0]) | (sizes[receiver] == 0), 0, jnp.maximum(slack, 0))
    moved = jax.random.randint(jax.random.fold_in(own, 4), (number_of // 2,), 0, 1 << 20) % (slack + 1)
    sizes = sizes.at[donor].add(-moved).at[receiver].add(moved)
    members = jnp.searchsorted(jnp.cumsum(sizes), jnp.arange(rows * top), side="right").astype(jnp.int32)
    grid = members.reshape(top, rows).T
    grid = grid[jax.random.permutation(jax.random.fold_in(own, 1), rows)]
    rotation = jax.random.randint(jax.random.fold_in(own, 2), (rows, 1), 0, top)
    return jnp.take_along_axis(grid, (jnp.arange(top)[None, :] + rotation) % top, axis=1)


def shares(count, total, bound, skew, full):
    weights = [(1 << 20) // math.isqrt(rank ** skew) + 1 for rank in range(1, count + 1)]
    largest = bound if full else min(bound, max(-(-total // count), total * weights[0] // sum(weights)))
    least = 1 if total - largest >= count - 1 else 0
    given, rest = [largest] + [least] * (count - 1), total - largest - least * (count - 1)
    while rest > 0:
        free = [i for i in range(1, count) if given[i] < largest] or [i for i in range(1, count) if given[i] < bound]
        pool, remaining = sum([weights[i] for i in free]), rest
        for i in free:
            addition = min(bound - given[i], max(1, remaining * weights[i] // pool), rest)
            given[i] = given[i] + addition
            rest = rest - addition
    return np.array(given)


def normal_values(key, extent, width, limit, split=(), kind=jnp.bfloat16):
    level = level_of(key, extent, split, -0.22, 0.18) if split else 1.0
    values = jax.random.normal(key, extent, jnp.float32) * width * level
    return jnp.minimum(jnp.maximum(values, -limit), limit).astype(kind)


def setup_inputs(seed: int = 0) -> dict:
    splits = jax.random.split(jax.random.key(seed), 15)
    conv_input = normal_values(splits[0], (TOKENS_A, D), 1.0, 6.0, ((0, 256),))
    conv_kernel = normal_values(splits[1], (KERNEL, D), KERNEL ** -0.5, 1.0, (), jnp.float32)
    conv_gain = jnp.clip(1.0 + 0.18 * jax.random.normal(splits[2], (D,), jnp.float32), 0.1, 1.9)
    out_weight = normal_values(splits[3], (D, D), D ** -0.5, 0.125, ((1, 4),))
    moe_input = normal_values(splits[4], (TOKENS_B, D), 1.0, 6.0, ((0, 256),))
    moe_gain = jnp.clip(1.0 + 0.18 * jax.random.normal(splits[5], (D,), jnp.float32), 0.1, 1.9)
    expert_gate = normal_values(splits[6], (EXPERTS, D, FF), D ** -0.5, 0.125, ((0, 64), (2, 4)))
    expert_up = normal_values(splits[7], (EXPERTS, D, FF), D ** -0.5, 0.125, ((0, 64), (2, 4)))
    expert_down = normal_values(splits[8], (EXPERTS, FF, D), FF ** -0.5, 0.125, ((0, 64), (1, 4)))
    shared_gate = normal_values(splits[9], (D, SHARED_FF), D ** -0.5, 0.125)
    shared_up = normal_values(splits[10], (D, SHARED_FF), D ** -0.5, 0.125)
    shared_down = normal_values(splits[11], (SHARED_FF, D), SHARED_FF ** -0.5, 0.5)
    expert_index_keys = jax.random.split(jax.random.fold_in(splits[12], 1), TOKENS_B // TOK_DEV_B)
    expert_index_turns = jax.random.permutation(jax.random.fold_in(splits[12], 3), TOKENS_B // TOK_DEV_B)
    expert_index = jax.vmap(lambda own, number: shared_out(jax.random.fold_in(splits[12], 2), own, number, TOK_DEV_B, EXPERTS, TOPK, SLOTS, 2))(expert_index_keys, expert_index_turns).reshape((TOKENS_B, TOPK))
    routing_weight = jnp.clip(0.25 + 1.25 * jax.random.uniform(splits[13], (TOKENS_B, TOPK), jnp.float32) ** level_of(splits[13], (TOKENS_B, TOPK), ((0, 256),), -0.2, 0.2), 0.25, 1.5)
    return dict(conv_input=conv_input, conv_kernel=conv_kernel, conv_gain=conv_gain, out_weight=out_weight, moe_input=moe_input, moe_gain=moe_gain, expert_gate=expert_gate, expert_up=expert_up, expert_down=expert_down, shared_gate=shared_gate, shared_up=shared_up, shared_down=shared_down, expert_index=expert_index, routing_weight=routing_weight)


NORM_EPS = 1e-05

def layer_scale(row_data, gain_vec):
    values = row_data.astype(jnp.float32)
    center = values - lax.optimization_barrier(jnp.mean(values, axis=-1, keepdims=True))
    spread = lax.optimization_barrier(jnp.mean(center * center, axis=-1, keepdims=True))
    return center * lax.rsqrt(spread + NORM_EPS) * gain_vec

def depthwise(padded, kernel, length):
    running = jnp.zeros((length, padded.shape[1]), jnp.float32)
    for offset in range(kernel.shape[0]):
        running = running + padded[offset:offset + length].astype(jnp.float32) * kernel[offset]
    return running

def slot_table(block_index, experts, slot_count):
    onehot = (block_index[:, :, None] == jnp.arange(experts, dtype=jnp.int32)[None, None, :]).astype(jnp.int32)
    before = jnp.cumsum(onehot, axis=1) - onehot
    position = lax.optimization_barrier(jnp.sum(before * onehot, axis=2))
    return (block_index * slot_count + position).astype(jnp.int32)

def reference(conv_input, conv_kernel, conv_gain, out_weight, moe_input, moe_gain, expert_gate, expert_up, expert_down, shared_gate, shared_up, shared_down, expert_index, routing_weight):
    length = conv_input.shape[0]
    padded = jnp.concatenate([jnp.zeros((KERNEL - 1, D), jnp.bfloat16), conv_input], axis=0)
    mixed_rows = depthwise(padded, conv_kernel, length)
    normed = jax.nn.silu(layer_scale(mixed_rows, conv_gain)).astype(jnp.bfloat16)
    conv_out = jnp.dot(normed, out_weight, preferred_element_type=jnp.float32).astype(jnp.bfloat16)
    normal = layer_scale(moe_input, moe_gain).astype(jnp.bfloat16)
    blocks = TOKENS_B // TOK_DEV_B
    entries = TOK_DEV_B * TOPK
    block_index = expert_index.reshape(blocks, entries)
    entry_slot = slot_table(block_index, EXPERTS, SLOTS)
    block_ids = jnp.arange(blocks, dtype=jnp.int32)[:, None]
    entry_row = block_ids * TOK_DEV_B + jnp.arange(entries, dtype=jnp.int32)[None, :] // TOPK
    slot_row = jnp.zeros((blocks, EXPERTS * SLOTS), jnp.int32).at[block_ids, entry_slot].set(entry_row)
    slot_weight = jnp.zeros((blocks, EXPERTS * SLOTS), jnp.float32).at[block_ids, entry_slot].set(routing_weight.reshape(blocks, entries))
    slot_row = slot_row.reshape(blocks, EXPERTS, SLOTS)
    slot_weight = slot_weight.reshape(blocks, EXPERTS, SLOTS)
    quarter = FF // N_TP

    def expert_step(running, expert_id):
        rows_of = lax.dynamic_index_in_dim(slot_row, expert_id, 1, keepdims=False).reshape(-1)
        weights = lax.dynamic_index_in_dim(slot_weight, expert_id, 1, keepdims=False).reshape(-1, 1)
        row_data = normal[rows_of]
        gate_proj = jnp.dot(row_data, expert_gate[expert_id], preferred_element_type=jnp.float32)
        up_proj = jnp.dot(row_data, expert_up[expert_id], preferred_element_type=jnp.float32)
        hidden = (jax.nn.silu(gate_proj) * up_proj).astype(jnp.bfloat16)
        down_all = expert_down[expert_id]
        summed = jnp.zeros((row_data.shape[0], D), jnp.float32)
        for index_q in range(N_TP):
            part_q = jnp.dot(hidden[:, index_q * quarter:(index_q + 1) * quarter], down_all[index_q * quarter:(index_q + 1) * quarter], preferred_element_type=jnp.float32).astype(jnp.bfloat16)
            summed = summed + lax.optimization_barrier(part_q).astype(jnp.float32)
        result = lax.optimization_barrier(summed.astype(jnp.bfloat16)).astype(jnp.float32)
        return (running.at[rows_of].add(weights * result), None)
    routed, _ = lax.scan(expert_step, jnp.zeros((TOKENS_B, D), jnp.float32), jnp.arange(EXPERTS, dtype=jnp.int32))
    shared_gate_proj = jnp.dot(normal, shared_gate, preferred_element_type=jnp.float32)
    shared_up_proj = jnp.dot(normal, shared_up, preferred_element_type=jnp.float32)
    shared_hidden = (jax.nn.silu(shared_gate_proj) * shared_up_proj).astype(jnp.bfloat16)
    shared_part = jnp.dot(shared_hidden, shared_down, preferred_element_type=jnp.float32)
    moe_out = (shared_part + routed).astype(jnp.bfloat16)
    return (conv_out, moe_out)
```

```python
import functools

import jax
import jax.numpy as jnp
from jax import lax
from jax.experimental import pallas as pl
from jax.experimental.pallas import tpu as pltpu
from jax.sharding import PartitionSpec as P

NORM_EPS = 1e-05
BF = jnp.bfloat16
F32 = jnp.float32
MESH_ID = pl.DeviceIdType.MESH
NZ, NX, NC, NY = 8, 4, 2, 4
NU = NX * NC
SL = 6
SLP = 8
CH = NU * SL
ROWS = 16


def remote(src, dst, send, recv, ep, tp):
    return pltpu.make_async_remote_copy(
        src_ref=src,
        dst_ref=dst,
        send_sem=send,
        recv_sem=recv,
        device_id=(ep, tp),
        device_id_type=MESH_ID,
    )


def shift_of(k):
    half = lax.div(k, 2)
    odd = lax.rem(k, 2)
    return odd * lax.rem(half + 1, 4) + (1 - odd) * (7 - half)


def silu(a):
    return a * lax.logistic(a)


def scaled(values, gain):
    center = values - jnp.mean(values, axis=-1, keepdims=True)
    spread = jnp.mean(center * center, axis=-1, keepdims=True)
    return center * lax.rsqrt(spread + NORM_EPS) * gain


def dot(a, b):
    return jnp.dot(a, b, preferred_element_type=F32)


def body(
    conv_in,
    conv_k,
    conv_g,
    ow_hbm,
    moe_in,
    moe_g,
    gate_hbm,
    up_hbm,
    down_hbm,
    sgate,
    sup,
    sdown,
    index,
    weight,
    conv_out,
    moe_out,
    ow,
    gate,
    up,
    down,
    halo,
    cpad,
    mixed,
    normed,
    tok,
    code_own,
    code_all,
    select,
    disp,
    xin,
    hid,
    part,
    rsa,
    rsb,
    ret,
    back,
    xs,
    xr,
    pick,
    shared,
    ld,
    halo_sem,
    tx_s,
    tx_r,
    code_s,
    code_r,
    cv_s,
    cv_r,
    zd_s,
    zd_r,
    ag_s,
    ag_r,
    rs_s,
    rs_r,
    zr_s,
    zr_r,
    xr_s,
    xr_r,
):
    tokens, width = moe_in.shape
    half = width // 2
    low, high = pl.ds(0, half), pl.ds(half, half)
    ep = lax.axis_index("ep")
    y = lax.axis_index("tp")
    z, u = lax.div(ep, NU), lax.rem(ep, NU)
    x, c = lax.div(u, NC), lax.rem(u, NC)
    yp, ym, yo = lax.rem(y + 1, NY), lax.rem(y + NY - 1, NY), lax.rem(y + 2, NY)

    def at_zu(zz, uu):
        return zz * NU + uu

    def at_xc(xx, cc):
        return z * NU + lax.rem(xx + NX, NX) * NC + cc

    flat = ep * NY + y
    count = NZ * NU * NY
    ahead = lax.rem(flat + 1, count)
    behind = lax.rem(flat + count - 1, count)

    barrier = pltpu.get_barrier_semaphore()

    def greet(e, t):
        pl.semaphore_signal(barrier, inc=1, device_id=(e, t), device_id_type=MESH_ID)

    greet(ep, yp)
    greet(ep, ym)
    for d in range(1, NZ):
        greet(at_zu(lax.rem(z + d, NZ), u), y)
    for d in range(1, NU):
        greet(at_zu(z, lax.rem(u + d, NU)), y)
    greet(lax.div(ahead, NY), lax.rem(ahead, NY))
    greet(lax.div(behind, NY), lax.rem(behind, NY))

    loads = [
        pltpu.make_async_copy(gate_hbm.at[0], gate, ld.at[0]),
        pltpu.make_async_copy(up_hbm.at[0], up, ld.at[1]),
        pltpu.make_async_copy(down_hbm.at[0], down, ld.at[2]),
        pltpu.make_async_copy(ow_hbm, ow, ld.at[3]),
    ]
    for load in loads:
        load.start()

    def norm_rows(r, _):
        rows = pl.ds(pl.multiple_of(r * ROWS, ROWS), ROWS)
        tok[u, rows, :] = scaled(moe_in[rows, :].astype(F32), moe_g[...]).astype(BF)
        return 0

    lax.fori_loop(0, tokens // ROWS, norm_rows, 0)

    own_index = index[pl.ds(pl.multiple_of(y * tokens, tokens), tokens), :]
    lane = lax.broadcasted_iota(jnp.int32, (tokens, 128), 1)
    expert = jnp.where(lane < NZ * NU, (lane & (NZ - 1)) * NU + (lane >> 3), -1)
    first = own_index[:, 0:1] == expert
    second = own_index[:, 1:2] == expert
    named = (first | second).astype(F32).astype(BF)
    row_i = lax.broadcasted_iota(jnp.int32, (tokens, tokens), 0)
    col_i = lax.broadcasted_iota(jnp.int32, (tokens, tokens), 1)
    earlier = (row_i < col_i).astype(F32).astype(BF)
    same = (row_i == col_i).astype(F32).astype(BF)
    over_tokens = (((0,), (0,)), ((), ()))
    named_t = lax.dot_general(named, same, over_tokens, preferred_element_type=F32)
    rank_t = lax.dot_general(named, earlier, over_tokens, preferred_element_type=F32)
    offset = (u * SL).astype(F32)
    code = jnp.where(named_t > 0.5, rank_t + offset, -1.0)
    for v in range(NU):
        code_own[v] = code[v * NZ : (v + 1) * NZ, :]
    rank = dot((row_i > col_i).astype(F32).astype(BF), named)
    slot_first = jnp.sum(jnp.where(first, rank, 0.0), axis=1, keepdims=True)
    slot_second = jnp.sum(jnp.where(second, rank, 0.0), axis=1, keepdims=True)
    place_first = own_index[:, 0:1] * SLP + slot_first.astype(jnp.int32)
    place_second = own_index[:, 1:2] * SLP + slot_second.astype(jnp.int32)
    place = lax.broadcasted_iota(jnp.int32, (tokens, NZ * NU * SLP), 1)
    pick[0:tokens, :] = (place == place_first).astype(F32).astype(BF)
    pick[tokens : 2 * tokens, :] = (place == place_second).astype(F32).astype(BF)

    pl.semaphore_wait(barrier, NZ - 1 + NU - 1 + 4)

    halo_copy = remote(
        conv_in.at[pl.ds(tokens - 32, 32), :],
        halo,
        halo_sem.at[0],
        halo_sem.at[1],
        lax.div(ahead, NY),
        lax.rem(ahead, NY),
    )
    halo_copy.start()

    def code_copy(d):
        v = lax.rem(u + d, NU)
        return remote(
            code_own.at[v], code_all.at[u], code_s.at[d], code_r.at[d], at_zu(z, v), y
        )

    def tok_copy(n, slot, columns, to):
        where = tok.at[slot, :, columns]
        return remote(where, where, tx_s.at[n], tx_r.at[n], to, y)

    u_of = lambda xx: lax.rem(xx + NX, NX) * NC + c
    xp, xm, mate = at_xc(x + 1, c), at_xc(x - 1, c), at_xc(x, 1 - c)
    every = pl.ds(0, width)
    tok_sends = [
        tok_copy(0, u, every, xp),
        tok_copy(1, u, every, xm),
        tok_copy(2, u_of(x - 1), low, xp),
        tok_copy(3, u_of(x + 1), high, xm),
        tok_copy(4, u, every, mate),
        tok_copy(5, u_of(x - 1), every, mate),
        tok_copy(6, u_of(x + 1), every, mate),
        tok_copy(7, u_of(x + 2), every, mate),
    ]

    def tok_wait(n, slot, columns):
        tok_copy(n, slot, columns, mate).wait_recv()

    mate_u = lambda xx: lax.rem(xx + NX, NX) * NC + 1 - c

    tok_sends[0].start()
    tok_sends[1].start()
    tok_sends[4].start()
    for d in range(1, NU):
        code_copy(d).start()

    blocks = width // 128

    def fill(b, _):
        columns = pl.ds(pl.multiple_of(b * 128, 128), 128)
        cpad[b, 32 : 32 + tokens, :] = conv_in[:, columns].astype(F32)
        return 0

    lax.fori_loop(0, blocks, fill, 0)
    halo_copy.wait_recv()
    keep = jnp.where(flat == 0, 0.0, 1.0)
    taps = conv_k.shape[0]

    def convolve(b, _):
        columns = pl.ds(pl.multiple_of(b * 128, 128), 128)
        cpad[b, 0:32, :] = halo[:, columns].astype(F32) * keep
        total = jnp.zeros((tokens, 128), F32)
        for k in range(taps):
            start = 33 - taps + k
            total = total + cpad[b, start : start + tokens, :] * conv_k[k : k + 1, columns]
        mixed[:, columns] = total
        return 0

    lax.fori_loop(0, blocks, convolve, 0)

    def conv_norm(r, _):
        rows = pl.ds(pl.multiple_of(r * ROWS, ROWS), ROWS)
        normed[y, rows, :] = silu(scaled(mixed[rows, :], conv_g[...])).astype(BF)
        return 0

    lax.fori_loop(0, tokens // ROWS, conv_norm, 0)

    def conv_copy(n, slot, columns, to):
        where = normed.at[slot, :, columns]
        return remote(where, where, cv_s.at[n], cv_r.at[n], ep, to)

    conv_sends = [
        conv_copy(0, y, every, yp),
        conv_copy(1, y, every, ym),
        conv_copy(2, ym, low, yp),
        conv_copy(3, yp, high, ym),
    ]
    conv_sends[0].start()
    conv_sends[1].start()

    tok_wait(0, u_of(x - 1), every)
    tok_sends[2].start()
    tok_sends[5].start()
    tok_wait(1, u_of(x + 1), every)
    tok_sends[3].start()
    tok_sends[6].start()
    conv_copy(0, ym, every, yp).wait_recv()
    conv_sends[2].start()
    conv_copy(1, yp, every, ym).wait_recv()
    conv_sends[3].start()
    for d in range(1, NU):
        v = lax.rem(u + NU - d, NU)
        remote(
            code_own.at[v], code_all.at[v], code_s.at[d], code_r.at[d], at_zu(z, v), y
        ).wait_recv()
    code_all[u] = code_own[u]
    slot_row = lax.broadcasted_iota(jnp.int32, (CH, tokens), 0).astype(F32)

    def build(v, _):
        columns = pl.ds(pl.multiple_of(v * tokens, tokens), tokens)
        codes = code_all[v]
        for zz in range(NZ):
            hit = slot_row == codes[zz : zz + 1, :]
            select[zz * CH : (zz + 1) * CH, columns] = hit.astype(F32).astype(BF)
        return 0

    lax.fori_loop(0, NU, build, 0)
    tok_wait(2, u_of(x + 2), low)
    tok_wait(3, u_of(x + 2), high)
    tok_sends[7].start()
    tok_wait(4, mate_u(x), every)
    tok_wait(5, mate_u(x - 1), every)
    tok_wait(6, mate_u(x + 1), every)
    tok_wait(7, mate_u(x + 2), every)

    wide = 512

    def gather(b, _):
        columns = pl.ds(pl.multiple_of(b * wide, wide), wide)
        rows = dot(select[...], tok[:, :, columns].reshape(NU * tokens, wide))
        disp[:, :, columns] = rows.astype(BF).reshape(NZ, CH, wide)
        return 0

    lax.fori_loop(0, width // wide, gather, 0)

    def disp_copy(k):
        target = lax.rem(z + shift_of(k), NZ)
        return remote(
            disp.at[target], xin.at[k, y], zd_s.at[k], zd_r.at[k], at_zu(target, u), y
        )

    def send_disp(k, _):
        disp_copy(k).start()
        return 0

    lax.fori_loop(0, NZ - 1, send_disp, 0)
    xin[NZ - 1, y] = disp[z]
    for load in loads:
        load.wait()

    def ag_copy(k, n, slot, columns, to):
        where = xin.at[k, slot, :, columns]
        return remote(where, where, ag_s.at[k, n], ag_r.at[k, n], ep, to)

    def ag_sends(k):
        return [
            ag_copy(k, 0, y, every, yp),
            ag_copy(k, 1, y, every, ym),
            ag_copy(k, 2, ym, low, yp),
            ag_copy(k, 3, yp, high, ym),
        ]

    def rs_sends(k):
        return [
            remote(part.at[k, yo, :, low], rsa.at[k, 0], rs_s.at[k, 0], rs_r.at[k, 0], ep, yp),
            remote(part.at[k, yo, :, high], rsa.at[k, 1], rs_s.at[k, 1], rs_r.at[k, 1], ep, ym),
            remote(part.at[k, yp], rsb.at[k, 0], rs_s.at[k, 2], rs_r.at[k, 2], ep, yp),
            remote(part.at[k, ym], rsb.at[k, 1], rs_s.at[k, 3], rs_r.at[k, 3], ep, ym),
        ]

    def ret_copy(k):
        source = lax.rem(z - shift_of(k) + NZ, NZ)
        return remote(ret.at[k], back.at[k], zr_s.at[k], zr_r.at[k], at_zu(source, u), y)

    def xr_copy(k, d):
        zz = lax.rem(z + shift_of(k), NZ)
        v = lax.rem(u + d, NU)
        return remote(
            xs.at[k, v], xr.at[zz, u], xr_s.at[k, d], xr_r.at[k, d], at_zu(z, v), y
        )

    def rows_out(k):
        @pl.when(k < NZ - 1)
        def _():
            disp_copy(k).wait_recv()

        sends = ag_sends(k)
        sends[0].start()
        sends[1].start()

    def rows_on(k):
        sends = ag_sends(k)
        ag_copy(k, 0, ym, every, yp).wait_recv()
        sends[2].start()
        ag_copy(k, 1, yp, every, ym).wait_recv()
        sends[3].start()

    def experts(k):
        ag_copy(k, 2, yo, low, yp).wait_recv()
        ag_copy(k, 3, yo, high, ym).wait_recv()
        rows = xin[k].reshape(NY * CH, width)
        ff = gate.shape[1]
        for b in range(ff // 256):
            columns = slice(b * 256, (b + 1) * 256)
            hid[:, columns] = (silu(dot(rows, gate[:, columns])) * dot(rows, up[:, columns])).astype(BF)

        def project(b, _):
            columns = pl.ds(pl.multiple_of(b * wide, wide), wide)
            out = dot(hid[...], down[:, columns]).astype(BF)
            part[k, :, :, columns] = out.reshape(NY, CH, wide)
            return 0

        lax.fori_loop(0, width // wide, project, 0)
        sends = rs_sends(k)
        sends[0].start()
        sends[1].start()

    def parts_on(k):
        sends = rs_sends(k)
        sends[0].wait_recv()
        kept = part[k, yp, :, low].astype(F32) + rsa[k, 0].astype(F32)
        part[k, yp, :, low] = kept.astype(BF)
        sends[2].start()
        sends[1].wait_recv()
        kept = part[k, ym, :, high].astype(F32) + rsa[k, 1].astype(F32)
        part[k, ym, :, high] = kept.astype(BF)
        sends[3].start()

    def results(k):
        sends = rs_sends(k)
        sends[2].wait_recv()
        sends[3].wait_recv()
        total = part[k, y].astype(F32) + rsb[k, 0].astype(F32) + rsb[k, 1].astype(F32)
        total = total.astype(BF)

        @pl.when(k < NZ - 1)
        def _():
            ret[k] = total
            ret_copy(k).start()

        @pl.when(k == NZ - 1)
        def _():
            back[k] = total

    spread_r = lax.broadcasted_iota(jnp.int32, (NU * SLP, CH), 0)
    spread_c = lax.broadcasted_iota(jnp.int32, (NU * SLP, CH), 1)
    spread = ((spread_r & 7) < SL) & (spread_c == (spread_r >> 3) * SL + (spread_r & 7))
    spread = spread.astype(F32).astype(BF)

    def results_home(k):
        @pl.when(k < NZ - 1)
        def _():
            ret_copy(k).wait_recv()

        def widen(b, _):
            columns = pl.ds(pl.multiple_of(b * wide, wide), wide)
            out = dot(spread, back[k, :, columns])
            xs[k, :, :, columns] = out.reshape(NU, SLP, wide).astype(BF)
            return 0

        lax.fori_loop(0, width // wide, widen, 0)

        def send(d, _):
            xr_copy(k, d).start()
            return 0

        lax.fori_loop(1, NU, send, 0)
        xr[lax.rem(z + shift_of(k), NZ), u] = xs[k, u]

    def beside():
        own = tok[u]
        hidden = (silu(dot(own, sgate[...])) * dot(own, sup[...])).astype(BF)
        shared[...] = dot(hidden, sdown[...])
        conv_copy(2, yo, low, yp).wait_recv()
        conv_copy(3, yo, high, ym).wait_recv()

        def project(b, _):
            rows = pl.ds(pl.multiple_of(b * tokens, tokens), tokens)
            conv_out[rows, :] = dot(normed[b], ow[...]).astype(BF)
            return 0

        lax.fori_loop(0, NY, project, 0)

    def stage(i, lag, act):
        k = i - lag

        @pl.when((k >= 0) & (k < NZ))
        def _():
            act(k)

    def step(i, _):
        stage(i, 0, rows_out)
        stage(i, 1, rows_on)
        stage(i, 2, experts)
        stage(i, 3, parts_on)
        stage(i, 4, results)
        stage(i, 5, results_home)

        @pl.when(i == 0)
        def _():
            beside()

        return 0

    lax.fori_loop(0, NZ + 5, step, 0)

    def arrived(k, _):
        zz = lax.rem(z + shift_of(k), NZ)

        def one(d, _):
            v = lax.rem(u + NU - d, NU)
            remote(
                xs.at[k, v], xr.at[zz, v], xr_s.at[k, d], xr_r.at[k, d], at_zu(z, v), y
            ).wait_recv()
            return 0

        lax.fori_loop(1, NU, one, 0)
        return 0

    lax.fori_loop(0, NZ, arrived, 0)

    def combine(b, _):
        columns = pl.ds(pl.multiple_of(b * wide, wide), wide)
        rows = xr[:, :, :, columns].astype(F32).reshape(NZ * NU * SLP, wide).astype(BF)
        both = dot(pick[...], rows)
        routed = both[0:tokens] * weight[:, 0:1] + both[tokens : 2 * tokens] * weight[:, 1:2]
        moe_out[:, columns] = (shared[:, columns] + routed).astype(BF)
        return 0

    lax.fori_loop(0, width // wide, combine, 0)

    halo_copy.wait_send()
    for copy in tok_sends + conv_sends:
        copy.wait_send()
    for d in range(1, NU):
        code_copy(d).wait_send()

    def drained(k, _):
        @pl.when(k < NZ - 1)
        def _():
            disp_copy(k).wait_send()
            ret_copy(k).wait_send()

        for copy in ag_sends(k) + rs_sends(k):
            copy.wait_send()

        def one(d, _):
            xr_copy(k, d).wait_send()
            return 0

        lax.fori_loop(1, NU, one, 0)
        return 0

    lax.fori_loop(0, NZ, drained, 0)


def on_device(*args):
    (
        conv_input,
        conv_kernel,
        conv_gain,
        out_weight,
        moe_input,
        moe_gain,
        expert_gate,
        expert_up,
        expert_down,
        shared_gate,
        shared_up,
        shared_down,
        expert_index,
        routing_weight,
    ) = args
    tokens, width = moe_input.shape
    half = width // 2
    ff = expert_gate.shape[2]
    cols = out_weight.shape[1]
    vm = lambda *shape, dtype=BF: pltpu.VMEM(shape, dtype)
    dma = lambda *shape: pltpu.SemaphoreType.DMA(shape)
    in_vmem = pl.BlockSpec(memory_space=pltpu.VMEM)
    in_hbm = pl.BlockSpec(memory_space=pl.ANY)
    operands = (
        (conv_input, in_vmem),
        (conv_kernel, in_vmem),
        (conv_gain.reshape(1, width), in_vmem),
        (out_weight, in_hbm),
        (moe_input, in_vmem),
        (moe_gain.reshape(1, width), in_vmem),
        (expert_gate, in_hbm),
        (expert_up, in_hbm),
        (expert_down, in_hbm),
        (shared_gate, in_vmem),
        (shared_up, in_vmem),
        (shared_down, in_vmem),
        (expert_index, in_vmem),
        (routing_weight, in_vmem),
    )
    scratch = [
        vm(width, cols),
        vm(width, ff),
        vm(width, ff),
        vm(ff, width),
        vm(32, width),
        vm(width // 128, 32 + tokens, 128, dtype=F32),
        vm(tokens, width, dtype=F32),
        vm(NY, tokens, width),
        vm(NU, tokens, width),
        vm(NU, NZ, tokens, dtype=F32),
        vm(NU, NZ, tokens, dtype=F32),
        vm(NZ * CH, NU * tokens),
        vm(NZ, CH, width),
        vm(NZ, NY, CH, width),
        vm(NY * CH, ff),
        vm(NZ, NY, CH, width),
        vm(NZ, 2, CH, half),
        vm(NZ, 2, CH, width),
        vm(NZ, CH, width),
        vm(NZ, CH, width),
        vm(NZ, NU, SLP, width),
        vm(NZ, NU, SLP, width),
        vm(2 * tokens, NZ * NU * SLP),
        vm(tokens, width, dtype=F32),
        dma(4),
        dma(2),
        dma(8),
        dma(8),
        dma(NU),
        dma(NU),
        dma(4),
        dma(4),
        dma(NZ),
        dma(NZ),
        dma(NZ, 4),
        dma(NZ, 4),
        dma(NZ, 4),
        dma(NZ, 4),
        dma(NZ),
        dma(NZ),
        dma(NZ, NU),
        dma(NZ, NU),
    ]
    return pl.pallas_call(
        body,
        out_shape=(
            jax.ShapeDtypeStruct((NY * tokens, cols), BF),
            jax.ShapeDtypeStruct((tokens, width), BF),
        ),
        in_specs=[spec for _, spec in operands],
        out_specs=(in_vmem, in_vmem),
        scratch_shapes=scratch,
        compiler_params=pltpu.CompilerParams(
            collective_id=0, has_side_effects=True, vmem_limit_bytes=67043328
        ),
    )(*[array for array, _ in operands])


def solution(mesh):
    in_specs = (
        P(("ep", "tp"), None),
        P(),
        P(),
        P(None, "tp"),
        P(("ep", "tp"), None),
        P(),
        P("ep", None, "tp"),
        P("ep", None, "tp"),
        P("ep", "tp", None),
        P(),
        P(),
        P(),
        P("ep", None),
        P(("ep", "tp"), None),
    )
    out_specs = (P("ep", "tp"), P(("ep", "tp"), None))
    return jax.shard_map(
        on_device, mesh=mesh, in_specs=in_specs, out_specs=out_specs, check_vma=False
    )
```

```python
import functools

import jax
import jax.numpy as jnp
from jax import lax
from jax.experimental import pallas as pl
from jax.experimental.pallas import tpu as pltpu
from jax.sharding import PartitionSpec as P

NORM_EPS = 1e-05
BF = jnp.bfloat16
F32 = jnp.float32
MESH_ID = pl.DeviceIdType.MESH
NZ, NU, NY = 8, 8, 4
SL = 6
SLP = 8
CH = NU * SL
ROWS = 16
EDGE = 32
HOME = 6
EARLY = 4


def remote(src, dst, send, recv, ep, tp):
    return pltpu.make_async_remote_copy(
        src_ref=src,
        dst_ref=dst,
        send_sem=send,
        recv_sem=recv,
        device_id=(ep, tp),
        device_id_type=MESH_ID,
    )


ORDER = (7, 2, 5, 3, 6, 4, 1, 0)
PACKED = sum(far << (4 * k) for k, far in enumerate(ORDER))


def shift_of(k):
    return lax.shift_right_logical(jnp.int32(PACKED), jnp.int32(4) * k) & 7


def silu(a):
    return a * lax.logistic(a)


def scaled(values, gain):
    center = values - jnp.mean(values, axis=-1, keepdims=True)
    spread = jnp.mean(center * center, axis=-1, keepdims=True)
    return center * lax.rsqrt(spread + NORM_EPS) * gain


def dot(a, b):
    return jnp.dot(a, b, preferred_element_type=F32)


def body(
    conv_hbm,
    taps_hbm,
    conv_g,
    ow_hbm,
    moe_hbm,
    moe_g,
    gate_hbm,
    up_hbm,
    down_hbm,
    sgate_hbm,
    sup_hbm,
    sdown_hbm,
    index,
    weight,
    conv_out,
    moe_out,
    conv_in,
    conv_k,
    moe_in,
    ow,
    gate,
    up,
    down,
    sgate,
    sup,
    sdown,
    halo,
    cpad,
    mixed,
    normed,
    own,
    xd,
    xdr,
    disp,
    xin,
    hid,
    part,
    rsa,
    rsb,
    ret,
    back,
    xs,
    xr,
    pick,
    shared,
    weights,
    ld,
    halo_sem,
    xd_s,
    xd_r,
    cv_s,
    cv_r,
    zd_s,
    zd_r,
    ag_s,
    ag_r,
    rs_s,
    rs_r,
    zr_s,
    zr_r,
    xr_s,
    xr_r,
):
    tokens, width = moe_in.shape
    half = width // 2
    wide = 512
    every, low, high = pl.ds(0, width), pl.ds(0, half), pl.ds(half, half)
    ep = lax.axis_index("ep")
    y = lax.axis_index("tp")
    z, u = lax.div(ep, NU), lax.rem(ep, NU)
    yp, ym, yo = lax.rem(y + 1, NY), lax.rem(y + NY - 1, NY), lax.rem(y + 2, NY)

    def at_zu(zz, uu):
        return zz * NU + uu

    flat = ep * NY + y
    count = NZ * NU * NY
    ahead = lax.rem(flat + 1, count)
    behind = lax.rem(flat + count - 1, count)

    barrier = pltpu.get_barrier_semaphore()

    def greet(e, t):
        pl.semaphore_signal(barrier, inc=1, device_id=(e, t), device_id_type=MESH_ID)

    greet(ep, yp)
    greet(ep, ym)
    for d in range(1, NZ):
        greet(at_zu(lax.rem(z + d, NZ), u), y)
    for d in range(1, NU):
        greet(at_zu(z, lax.rem(u + d, NU)), y)
    greet(lax.div(ahead, NY), lax.rem(ahead, NY))
    greet(lax.div(behind, NY), lax.rem(behind, NY))

    loads = [
        pltpu.make_async_copy(source, target, ld.at[n])
        for n, (source, target) in enumerate(
            (
                (moe_hbm, moe_in),
                (conv_hbm, conv_in),
                (taps_hbm, conv_k),
                (gate_hbm.at[0], gate),
                (up_hbm.at[0], up),
                (down_hbm.at[0], down),
                (ow_hbm, ow),
                (sgate_hbm, sgate),
                (sup_hbm, sup),
                (sdown_hbm, sdown),
            )
        )
    ]
    for load in loads:
        load.start()

    mine = index[:, pl.ds(pl.multiple_of(y * tokens, tokens), tokens)]
    expert = lax.broadcasted_iota(jnp.int32, (NZ * NU, tokens), 0)
    first = expert == mine[0:1, :]
    second = expert == mine[1:2, :]
    named = (first | second).astype(F32).astype(BF)
    row_i = lax.broadcasted_iota(jnp.int32, (tokens, tokens), 0)
    col_i = lax.broadcasted_iota(jnp.int32, (tokens, tokens), 1)
    rank = dot(named, (row_i < col_i).astype(F32).astype(BF))
    rank_first = jnp.sum(jnp.where(first, rank, 0.0), axis=0, keepdims=True)
    rank_second = jnp.sum(jnp.where(second, rank, 0.0), axis=0, keepdims=True)
    place_first = mine[0:1, :] * SLP + rank_first.astype(jnp.int32)
    place_second = mine[1:2, :] * SLP + rank_second.astype(jnp.int32)
    place = lax.broadcasted_iota(jnp.int32, (NZ * NU * SLP, tokens), 0)
    select = ((place == place_first) | (place == place_second)).astype(F32).astype(BF)

    share = weight[...]
    share_a = share.astype(BF).astype(F32)
    share_b = (share - share_a).astype(BF).astype(F32)
    share_c = share - share_a - share_b
    line = lax.broadcasted_iota(jnp.int32, (16, tokens), 0)
    table = jnp.zeros((16, tokens), F32)
    for n, values in enumerate(
        (
            mine[0:1, :].astype(F32),
            mine[1:2, :].astype(F32),
            rank_first,
            rank_second,
            share_a[0:1, :],
            share_a[1:2, :],
            share_b[0:1, :],
            share_b[1:2, :],
            share_c[0:1, :],
            share_c[1:2, :],
        )
    ):
        table = jnp.where(line == n, values, table)
    turned = lax.dot_general(
        (row_i == col_i).astype(F32).astype(BF),
        table.astype(BF),
        (((1,), (1,)), ((), ())),
        preferred_element_type=F32,
    )
    weights[:, 0:2] = turned[:, 4:6] + turned[:, 6:8] + turned[:, 8:10]
    places = (turned[:, 0:2] * SLP + turned[:, 2:4]).astype(jnp.int32)
    spot = lax.broadcasted_iota(jnp.int32, (tokens, NZ * NU * SLP), 1)
    pick[0:tokens, :] = (spot == places[:, 0:1]).astype(F32).astype(BF)
    pick[tokens : 2 * tokens, :] = (spot == places[:, 1:2]).astype(F32).astype(BF)

    loads[0].wait()

    def norm_rows(r, _):
        rows = pl.ds(pl.multiple_of(r * ROWS, ROWS), ROWS)
        own[rows, :] = scaled(moe_in[rows, :].astype(F32), moe_g[...]).astype(BF)
        return 0

    lax.fori_loop(0, tokens // ROWS, norm_rows, 0)

    def gather(b, _):
        columns = pl.ds(pl.multiple_of(b * wide, wide), wide)
        rows = dot(select, own[:, columns])
        xd[:, :, :, columns] = rows.reshape(NZ, NU, SLP, wide).astype(BF)
        return 0

    lax.fori_loop(0, width // wide, gather, 0)

    blocks = width // 128
    taps = conv_k.shape[0]
    loads[1].wait()
    loads[2].wait()

    def fill(b, _):
        columns = pl.ds(pl.multiple_of(b * 128, 128), 128)
        cpad[b, EDGE : EDGE + tokens, :] = conv_in[:, columns].astype(F32)
        return 0

    lax.fori_loop(0, blocks, fill, 0)

    def convolve(begin, length):
        def one(b, _):
            columns = pl.ds(pl.multiple_of(b * 128, 128), 128)
            total = jnp.zeros((length, 128), F32)
            for k in range(taps):
                start = begin + EDGE + 1 - taps + k
                total = total + cpad[b, start : start + length, :] * conv_k[k : k + 1, columns]
            mixed[begin : begin + length, columns] = total
            return 0

        lax.fori_loop(0, blocks, one, 0)

        def conv_norm(r, _):
            rows = pl.ds(pl.multiple_of(begin + r * ROWS, ROWS), ROWS)
            normed[y, rows, :] = silu(scaled(mixed[rows, :], conv_g[...])).astype(BF)
            return 0

        lax.fori_loop(0, length // ROWS, conv_norm, 0)

    def conv_copy(n, slot, columns, to):
        rows = pl.ds(EDGE, tokens - EDGE) if n < 4 else pl.ds(0, EDGE)
        where = normed.at[slot, rows, columns]
        return remote(where, where, cv_s.at[n], cv_r.at[n], ep, to)

    conv_sends = [
        conv_copy(0, y, every, yp),
        conv_copy(1, y, every, ym),
        conv_copy(2, ym, low, yp),
        conv_copy(3, yp, high, ym),
        conv_copy(4, y, every, yp),
        conv_copy(5, y, every, ym),
        conv_copy(6, ym, low, yp),
        conv_copy(7, yp, high, ym),
    ]
    convolve(EDGE, tokens - EDGE)

    pl.semaphore_wait(barrier, NZ - 1 + NU - 1 + 4)

    halo_copy = remote(
        conv_in.at[pl.ds(tokens - EDGE, EDGE), :],
        halo,
        halo_sem.at[0],
        halo_sem.at[1],
        lax.div(ahead, NY),
        lax.rem(ahead, NY),
    )
    halo_copy.start()

    def xd_copy(k, d):
        zz = lax.rem(z + shift_of(k), NZ)
        v = lax.rem(u + d, NU)
        return remote(
            xd.at[zz, v], xdr.at[zz, u], xd_s.at[k, d], xd_r.at[k, d], at_zu(z, v), y
        )

    def send_rows(k, _):
        def one(d, _):
            xd_copy(k, d).start()
            return 0

        return lax.fori_loop(1, NU, one, 0)

    send_rows(0, 0)
    conv_sends[0].start()
    conv_sends[1].start()
    lax.fori_loop(1, NZ, send_rows, 0)

    halo_copy.wait_recv()
    keep = jnp.where(flat == 0, 0.0, 1.0)

    def fill_edge(b, _):
        columns = pl.ds(pl.multiple_of(b * 128, 128), 128)
        cpad[b, 0:EDGE, :] = halo[:, columns].astype(F32) * keep
        return 0

    lax.fori_loop(0, blocks, fill_edge, 0)
    convolve(0, EDGE)
    conv_sends[4].start()
    conv_sends[5].start()

    wide_r = lax.broadcasted_iota(jnp.int32, (NU * SLP, CH), 0)
    wide_c = lax.broadcasted_iota(jnp.int32, (NU * SLP, CH), 1)
    spread = ((wide_r & 7) < SL) & (wide_c == (wide_r >> 3) * SL + (wide_r & 7))
    spread = spread.astype(F32).astype(BF)
    pack_r = lax.broadcasted_iota(jnp.int32, (CH, NU * SLP), 0)
    pack_c = lax.broadcasted_iota(jnp.int32, (CH, NU * SLP), 1)
    pack = ((pack_c & 7) < SL) & (pack_r == (pack_c >> 3) * SL + (pack_c & 7))
    pack = pack.astype(F32).astype(BF)

    def disp_copy(k):
        target = lax.rem(z + shift_of(k), NZ)
        return remote(
            disp.at[k], xin.at[k, y], zd_s.at[k], zd_r.at[k], at_zu(target, u), y
        )

    def rows_along(k):
        zz = lax.rem(z + shift_of(k), NZ)

        def one(d, _):
            v = lax.rem(u + NU - d, NU)
            remote(
                xd.at[zz, v], xdr.at[zz, v], xd_s.at[k, d], xd_r.at[k, d], at_zu(z, v), y
            ).wait_recv()
            return 0

        lax.fori_loop(1, NU, one, 0)
        xdr[zz, u] = xd[zz, u]

        def narrow(b, _):
            columns = pl.ds(pl.multiple_of(b * wide, wide), wide)
            rows = xdr[zz, :, :, columns].astype(F32).reshape(NU * SLP, wide).astype(BF)
            rows = dot(pack, rows).astype(BF)

            @pl.when(k < NZ - 1)
            def _():
                disp[k, :, columns] = rows

            @pl.when(k == NZ - 1)
            def _():
                xin[k, y, :, columns] = rows

            return 0

        lax.fori_loop(0, width // wide, narrow, 0)

        @pl.when(k < NZ - 1)
        def _():
            disp_copy(k).start()

    def rows_first(k, _):
        rows_along(k)
        return 0

    lax.fori_loop(0, 2, rows_first, 0)
    conv_copy(0, ym, every, yp).wait_recv()
    conv_sends[2].start()
    conv_copy(1, yp, every, ym).wait_recv()
    conv_sends[3].start()
    lax.fori_loop(2, 3, rows_first, 0)
    conv_copy(4, ym, every, yp).wait_recv()
    conv_sends[6].start()
    conv_copy(5, yp, every, ym).wait_recv()
    conv_sends[7].start()
    lax.fori_loop(3, EARLY, rows_first, 0)
    for load in loads[3:]:
        load.wait()

    def ag_copy(k, n, slot, columns, to):
        where = xin.at[k, slot, :, columns]
        return remote(where, where, ag_s.at[k, n], ag_r.at[k, n], ep, to)

    def ag_sends(k):
        return [
            ag_copy(k, 0, y, every, yp),
            ag_copy(k, 1, y, every, ym),
            ag_copy(k, 2, ym, low, yp),
            ag_copy(k, 3, yp, high, ym),
        ]

    def rs_sends(k):
        return [
            remote(part.at[k, yo, :, low], rsa.at[k, 0], rs_s.at[k, 0], rs_r.at[k, 0], ep, yp),
            remote(part.at[k, yo, :, high], rsa.at[k, 1], rs_s.at[k, 1], rs_r.at[k, 1], ep, ym),
            remote(part.at[k, yp], rsb.at[k, 0], rs_s.at[k, 2], rs_r.at[k, 2], ep, yp),
            remote(part.at[k, ym], rsb.at[k, 1], rs_s.at[k, 3], rs_r.at[k, 3], ep, ym),
        ]

    def ret_copy(k):
        source = lax.rem(z - shift_of(k) + NZ, NZ)
        return remote(ret.at[k], back.at[k], zr_s.at[k], zr_r.at[k], at_zu(source, u), y)

    def xr_copy(k, d):
        zz = lax.rem(z + shift_of(k), NZ)
        v = lax.rem(u + d, NU)
        return remote(
            xs.at[k, v], xr.at[zz, u], xr_s.at[k, d], xr_r.at[k, d], at_zu(z, v), y
        )

    def rows_out(k):
        @pl.when(k < NZ - 1)
        def _():
            disp_copy(k).wait_recv()

        sends = ag_sends(k)
        sends[0].start()
        sends[1].start()

    def rows_on(k):
        sends = ag_sends(k)
        ag_copy(k, 0, ym, every, yp).wait_recv()
        sends[2].start()
        ag_copy(k, 1, yp, every, ym).wait_recv()
        sends[3].start()

    def experts(k):
        ag_copy(k, 2, yo, low, yp).wait_recv()
        ag_copy(k, 3, yo, high, ym).wait_recv()
        rows = xin[k].reshape(NY * CH, width)
        ff = gate.shape[1]
        for b in range(ff // 256):
            columns = slice(b * 256, (b + 1) * 256)
            hid[:, columns] = (silu(dot(rows, gate[:, columns])) * dot(rows, up[:, columns])).astype(BF)

        def project(b, _):
            columns = pl.ds(pl.multiple_of(b * wide, wide), wide)
            out = dot(hid[...], down[:, columns]).astype(BF)
            part[k, :, :, columns] = out.reshape(NY, CH, wide)
            return 0

        lax.fori_loop(0, width // wide, project, 0)
        sends = rs_sends(k)
        sends[0].start()
        sends[1].start()

    def parts_on(k):
        sends = rs_sends(k)
        sends[0].wait_recv()
        kept = part[k, yp, :, low].astype(F32) + rsa[k, 0].astype(F32)
        part[k, yp, :, low] = kept.astype(BF)
        sends[2].start()
        sends[1].wait_recv()
        kept = part[k, ym, :, high].astype(F32) + rsa[k, 1].astype(F32)
        part[k, ym, :, high] = kept.astype(BF)
        sends[3].start()

    def results(k):
        sends = rs_sends(k)
        sends[2].wait_recv()
        sends[3].wait_recv()
        total = part[k, y].astype(F32) + rsb[k, 0].astype(F32) + rsb[k, 1].astype(F32)
        total = total.astype(BF)

        @pl.when(k < NZ - 1)
        def _():
            ret[k] = total
            ret_copy(k).start()

        @pl.when(k == NZ - 1)
        def _():
            back[k] = total

    def results_home(k):
        @pl.when(k < NZ - 1)
        def _():
            ret_copy(k).wait_recv()

        def widen(b, _):
            columns = pl.ds(pl.multiple_of(b * wide, wide), wide)
            out = dot(spread, back[k, :, columns])
            xs[k, :, :, columns] = out.reshape(NU, SLP, wide).astype(BF)
            return 0

        lax.fori_loop(0, width // wide, widen, 0)

        def send(d, _):
            xr_copy(k, d).start()
            return 0

        lax.fori_loop(1, NU, send, 0)
        xr[lax.rem(z + shift_of(k), NZ), u] = xs[k, u]

    def beside():
        rows = own[...]
        hidden = (silu(dot(rows, sgate[...])) * dot(rows, sup[...])).astype(BF)
        shared[...] = dot(hidden, sdown[...])
        conv_copy(2, yo, low, yp).wait_recv()
        conv_copy(3, yo, high, ym).wait_recv()
        conv_copy(6, yo, low, yp).wait_recv()
        conv_copy(7, yo, high, ym).wait_recv()

        def project(b, _):
            rows = pl.ds(pl.multiple_of(b * tokens, tokens), tokens)
            conv_out[rows, :] = dot(normed[b], ow[...]).astype(BF)
            return 0

        lax.fori_loop(0, NY, project, 0)

    def stage(i, lag, act):
        k = i - lag

        @pl.when((k >= 0) & (k < NZ))
        def _():
            act(k)

    def step(i, _):
        stage(i, 0, rows_out)
        stage(i, 1, rows_on)
        stage(i, 2, experts)
        stage(i, 3, parts_on)
        stage(i, 4, results)
        stage(i, -EARLY, rows_along)
        stage(i, HOME, results_home)

        @pl.when(i == 1)
        def _():
            beside()

        return 0

    lax.fori_loop(0, NZ + HOME, step, 0)

    def arrived(k, _):
        zz = lax.rem(z + shift_of(k), NZ)

        def one(d, _):
            v = lax.rem(u + NU - d, NU)
            remote(
                xs.at[k, v], xr.at[zz, v], xr_s.at[k, d], xr_r.at[k, d], at_zu(z, v), y
            ).wait_recv()
            return 0

        lax.fori_loop(1, NU, one, 0)
        return 0

    lax.fori_loop(0, NZ, arrived, 0)

    def combine(b, _):
        columns = pl.ds(pl.multiple_of(b * wide, wide), wide)
        rows = xr[:, :, :, columns].astype(F32).reshape(NZ * NU * SLP, wide).astype(BF)
        both = dot(pick[...], rows)
        routed = both[0:tokens] * weights[:, 0:1] + both[tokens : 2 * tokens] * weights[:, 1:2]
        moe_out[:, columns] = (shared[:, columns] + routed).astype(BF)
        return 0

    lax.fori_loop(0, width // wide, combine, 0)

    halo_copy.wait_send()
    for copy in conv_sends:
        copy.wait_send()

    def drained(k, _):
        @pl.when(k < NZ - 1)
        def _():
            disp_copy(k).wait_send()
            ret_copy(k).wait_send()

        for copy in ag_sends(k) + rs_sends(k):
            copy.wait_send()

        def one(d, _):
            xd_copy(k, d).wait_send()
            xr_copy(k, d).wait_send()
            return 0

        lax.fori_loop(1, NU, one, 0)
        return 0

    lax.fori_loop(0, NZ, drained, 0)


def on_device(*args):
    (
        conv_input,
        conv_kernel,
        conv_gain,
        out_weight,
        moe_input,
        moe_gain,
        expert_gate,
        expert_up,
        expert_down,
        shared_gate,
        shared_up,
        shared_down,
        expert_index,
        routing_weight,
    ) = args
    tokens, width = moe_input.shape
    half = width // 2
    ff = expert_gate.shape[2]
    cols = out_weight.shape[1]
    vm = lambda *shape, dtype=BF: pltpu.VMEM(shape, dtype)
    dma = lambda *shape: pltpu.SemaphoreType.DMA(shape)
    in_vmem = pl.BlockSpec(memory_space=pltpu.VMEM)
    in_hbm = pl.BlockSpec(memory_space=pl.ANY)
    operands = (
        (conv_input, in_hbm),
        (conv_kernel, in_hbm),
        (conv_gain.reshape(1, width), in_vmem),
        (out_weight, in_hbm),
        (moe_input, in_hbm),
        (moe_gain.reshape(1, width), in_vmem),
        (expert_gate, in_hbm),
        (expert_up, in_hbm),
        (expert_down, in_hbm),
        (shared_gate, in_hbm),
        (shared_up, in_hbm),
        (shared_down, in_hbm),
        (expert_index.T, in_vmem),
        (routing_weight.T, in_vmem),
    )
    scratch = [
        vm(tokens, width),
        vm(*conv_kernel.shape, dtype=F32),
        vm(tokens, width),
        vm(width, cols),
        vm(width, ff),
        vm(width, ff),
        vm(ff, width),
        vm(*shared_gate.shape),
        vm(*shared_up.shape),
        vm(*shared_down.shape),
        vm(EDGE, width),
        vm(width // 128, EDGE + tokens, 128, dtype=F32),
        vm(tokens, width, dtype=F32),
        vm(NY, tokens, width),
        vm(tokens, width),
        vm(NZ, NU, SLP, width),
        vm(NZ, NU, SLP, width),
        vm(NZ, CH, width),
        vm(NZ, NY, CH, width),
        vm(NY * CH, ff),
        vm(NZ, NY, CH, width),
        vm(NZ, 2, CH, half),
        vm(NZ, 2, CH, width),
        vm(NZ, CH, width),
        vm(NZ, CH, width),
        vm(NZ, NU, SLP, width),
        vm(NZ, NU, SLP, width),
        vm(2 * tokens, NZ * NU * SLP),
        vm(tokens, width, dtype=F32),
        vm(tokens, 128, dtype=F32),
        dma(10),
        dma(2),
        dma(NZ, NU),
        dma(NZ, NU),
        dma(8),
        dma(8),
        dma(NZ),
        dma(NZ),
        dma(NZ, 4),
        dma(NZ, 4),
        dma(NZ, 4),
        dma(NZ, 4),
        dma(NZ),
        dma(NZ),
        dma(NZ, NU),
        dma(NZ, NU),
    ]
    return pl.pallas_call(
        body,
        out_shape=(
            jax.ShapeDtypeStruct((NY * tokens, cols), BF),
            jax.ShapeDtypeStruct((tokens, width), BF),
        ),
        in_specs=[spec for _, spec in operands],
        out_specs=(in_vmem, in_vmem),
        scratch_shapes=scratch,
        compiler_params=pltpu.CompilerParams(
            collective_id=0, has_side_effects=True, vmem_limit_bytes=67043328
        ),
    )(*[array for array, _ in operands])


def solution(mesh):
    in_specs = (
        P(("ep", "tp"), None),
        P(),
        P(),
        P(None, "tp"),
        P(("ep", "tp"), None),
        P(),
        P("ep", None, "tp"),
        P("ep", None, "tp"),
        P("ep", "tp", None),
        P(),
        P(),
        P(),
        P("ep", None),
        P(("ep", "tp"), None),
    )
    out_specs = (P("ep", "tp"), P(("ep", "tp"), None))
    return jax.shard_map(
        on_device, mesh=mesh, in_specs=in_specs, out_specs=out_specs, check_vma=False
    )
```

```python
import functools

import jax
import jax.numpy as jnp
from jax import lax
from jax.experimental import pallas as pl
from jax.experimental.pallas import tpu as pltpu
from jax.sharding import PartitionSpec as P

NORM_EPS = 1e-05
BF = jnp.bfloat16
F32 = jnp.float32
MESH_ID = pl.DeviceIdType.MESH
NZ, NU, NY = 8, 8, 4
SL = 6
SLP = 8
CH = NU * SL
ROWS = 16
EDGE = 32
HOME = 6
PACE = 3
EARLY = 4


def remote(src, dst, send, recv, ep, tp):
    return pltpu.make_async_remote_copy(
        src_ref=src,
        dst_ref=dst,
        send_sem=send,
        recv_sem=recv,
        device_id=(ep, tp),
        device_id_type=MESH_ID,
    )


ORDER = (2, 6, 5, 3, 4, 7, 1, 0)
LOCAL = ORDER.index(0)
PACKED = sum(far << (4 * k) for k, far in enumerate(ORDER))


def shift_of(k):
    return lax.shift_right_logical(jnp.int32(PACKED), jnp.int32(4) * k) & 7


def silu(a):
    return a * lax.logistic(a)


def scaled(values, gain):
    center = values - jnp.mean(values, axis=-1, keepdims=True)
    spread = jnp.mean(center * center, axis=-1, keepdims=True)
    return center * lax.rsqrt(spread + NORM_EPS) * gain


def dot(a, b):
    return jnp.dot(a, b, preferred_element_type=F32)


def body(
    conv_hbm,
    taps_hbm,
    conv_g_hbm,
    ow_hbm,
    moe_hbm,
    moe_g_hbm,
    gate_hbm,
    up_hbm,
    down_hbm,
    sgate_hbm,
    sup_hbm,
    sdown_hbm,
    index_hbm,
    weight_hbm,
    conv_out,
    moe_out,
    conv_in,
    conv_k,
    conv_g,
    moe_in,
    moe_g,
    index,
    weight,
    ow,
    gate,
    up,
    down,
    sgate,
    sup,
    sdown,
    halo,
    cpad,
    mixed,
    normed,
    own,
    select,
    xd,
    xdr,
    disp,
    xin,
    hid,
    part,
    rsa,
    rsb,
    ret,
    back,
    xs,
    xr,
    pick,
    shared,
    weights,
    conv_held,
    moe_held,
    ld,
    halo_sem,
    xd_s,
    xd_r,
    cv_s,
    cv_r,
    zd_s,
    zd_r,
    ag_s,
    ag_r,
    rs_s,
    rs_r,
    zr_s,
    zr_r,
    xr_s,
    xr_r,
    out_sem,
):
    tokens, width = moe_in.shape
    half = width // 2
    wide = 512
    every, low, high = pl.ds(0, width), pl.ds(0, half), pl.ds(half, half)
    ep = lax.axis_index("ep")
    y = lax.axis_index("tp")
    z, u = lax.div(ep, NU), lax.rem(ep, NU)
    yp, ym, yo = lax.rem(y + 1, NY), lax.rem(y + NY - 1, NY), lax.rem(y + 2, NY)

    def at_zu(zz, uu):
        return zz * NU + uu

    flat = ep * NY + y
    count = NZ * NU * NY
    ahead = lax.rem(flat + 1, count)
    behind = lax.rem(flat + count - 1, count)

    barrier = pltpu.get_barrier_semaphore()

    def greet(e, t):
        pl.semaphore_signal(barrier, inc=1, device_id=(e, t), device_id_type=MESH_ID)

    greet(ep, yp)
    greet(ep, ym)
    for d in range(1, NZ):
        greet(at_zu(lax.rem(z + d, NZ), u), y)
    for d in range(1, NU):
        greet(at_zu(z, lax.rem(u + d, NU)), y)
    greet(lax.div(ahead, NY), lax.rem(ahead, NY))
    greet(lax.div(behind, NY), lax.rem(behind, NY))

    loads = [
        pltpu.make_async_copy(source, target, ld.at[n])
        for n, (source, target) in enumerate(
            (
                (conv_hbm, conv_in),
                (taps_hbm, conv_k),
                (conv_g_hbm, conv_g),
                (index_hbm, index),
                (weight_hbm, weight),
                (moe_hbm, moe_in),
                (moe_g_hbm, moe_g),
                (gate_hbm.at[0], gate),
                (up_hbm.at[0], up),
                (down_hbm.at[0], down),
                (ow_hbm, ow),
                (sgate_hbm, sgate),
                (sup_hbm, sup),
                (sdown_hbm, sdown),
            )
        )
    ]
    for load in loads:
        load.start()

    blocks = width // 128
    taps = conv_k.shape[0]
    for load in loads[0:3]:
        load.wait()

    def fill(b, _):
        columns = pl.ds(pl.multiple_of(b * 128, 128), 128)
        cpad[b, EDGE : EDGE + tokens, :] = conv_in[:, columns].astype(F32)
        return 0

    lax.fori_loop(0, blocks, fill, 0)

    def convolve(begin, length):
        def one(b, _):
            columns = pl.ds(pl.multiple_of(b * 128, 128), 128)
            total = jnp.zeros((length, 128), F32)
            for k in range(taps):
                start = begin + EDGE + 1 - taps + k
                total = total + cpad[b, start : start + length, :] * conv_k[k : k + 1, columns]
            mixed[begin : begin + length, columns] = total
            return 0

        lax.fori_loop(0, blocks, one, 0)

        def conv_norm(r, _):
            rows = pl.ds(pl.multiple_of(begin + r * ROWS, ROWS), ROWS)
            normed[y, rows, :] = silu(scaled(mixed[rows, :], conv_g[...])).astype(BF)
            return 0

        lax.fori_loop(0, length // ROWS, conv_norm, 0, unroll=2)

    def conv_copy(n, slot, columns, to):
        rows = pl.ds(EDGE, tokens - EDGE) if n < 4 else pl.ds(0, EDGE)
        where = normed.at[slot, rows, columns]
        return remote(where, where, cv_s.at[0], cv_r.at[n], ep, to)

    conv_sends = [
        conv_copy(0, y, every, yp),
        conv_copy(1, y, every, ym),
        conv_copy(2, ym, low, yp),
        conv_copy(3, yp, high, ym),
        conv_copy(4, y, every, yp),
        conv_copy(5, y, every, ym),
        conv_copy(6, ym, low, yp),
        conv_copy(7, yp, high, ym),
    ]
    convolve(EDGE, tokens - EDGE)

    pl.semaphore_wait(barrier, NZ - 1 + NU - 1 + 4)

    halo_copy = remote(
        conv_in.at[pl.ds(tokens - EDGE, EDGE), :],
        halo,
        halo_sem.at[0],
        halo_sem.at[1],
        lax.div(ahead, NY),
        lax.rem(ahead, NY),
    )
    halo_copy.start()
    conv_sends[0].start()
    conv_sends[1].start()

    loads[3].wait()
    loads[4].wait()

    mine = index[:, pl.ds(pl.multiple_of(y * tokens, tokens), tokens)]
    expert = lax.broadcasted_iota(jnp.int32, (NZ * NU, tokens), 0)
    first = expert == mine[0:1, :]
    second = expert == mine[1:2, :]
    named = (first | second).astype(F32).astype(BF)
    row_i = lax.broadcasted_iota(jnp.int32, (tokens, tokens), 0)
    col_i = lax.broadcasted_iota(jnp.int32, (tokens, tokens), 1)
    rank = dot(named, (row_i < col_i).astype(F32).astype(BF))
    rank_first = jnp.sum(jnp.where(first, rank, 0.0), axis=0, keepdims=True)
    rank_second = jnp.sum(jnp.where(second, rank, 0.0), axis=0, keepdims=True)
    place_first = mine[0:1, :] * SLP + rank_first.astype(jnp.int32)
    place_second = mine[1:2, :] * SLP + rank_second.astype(jnp.int32)
    place = lax.broadcasted_iota(jnp.int32, (NZ * NU * SLP, tokens), 0)
    hits = ((place == place_first) | (place == place_second)).astype(F32).astype(BF)
    select[...] = hits.reshape(NZ, NU * SLP, tokens)

    share = weight[...]
    share_a = share.astype(BF).astype(F32)
    share_b = (share - share_a).astype(BF).astype(F32)
    share_c = share - share_a - share_b
    line = lax.broadcasted_iota(jnp.int32, (16, tokens), 0)
    table = jnp.zeros((16, tokens), F32)
    for n, values in enumerate(
        (
            mine[0:1, :].astype(F32),
            mine[1:2, :].astype(F32),
            rank_first,
            rank_second,
            share_a[0:1, :],
            share_a[1:2, :],
            share_b[0:1, :],
            share_b[1:2, :],
            share_c[0:1, :],
            share_c[1:2, :],
        )
    ):
        table = jnp.where(line == n, values, table)
    turned = lax.dot_general(
        (row_i == col_i).astype(F32).astype(BF),
        table.astype(BF),
        (((1,), (1,)), ((), ())),
        preferred_element_type=F32,
    )
    weights[:, 0:2] = turned[:, 4:6] + turned[:, 6:8] + turned[:, 8:10]
    places = (turned[:, 0:2] * SLP + turned[:, 2:4]).astype(jnp.int32)
    spot = lax.broadcasted_iota(jnp.int32, (tokens, NZ * NU * SLP), 1)
    pick[0:tokens, :] = (spot == places[:, 0:1]).astype(F32).astype(BF)
    pick[tokens : 2 * tokens, :] = (spot == places[:, 1:2]).astype(F32).astype(BF)

    loads[5].wait()
    loads[6].wait()

    def norm_rows(r, _):
        rows = pl.ds(pl.multiple_of(r * ROWS, ROWS), ROWS)
        own[rows, :] = scaled(moe_in[rows, :].astype(F32), moe_g[...]).astype(BF)
        return 0

    lax.fori_loop(0, tokens // ROWS, norm_rows, 0, unroll=4)

    def xd_copy(k, d):
        zz = lax.rem(z + shift_of(k), NZ)
        v = lax.rem(u + d, NU)
        return remote(
            xd.at[zz, v], xdr.at[zz, u], xd_s.at[0], xd_r.at[k], at_zu(z, v), y
        )

    def send_rows(k, _):
        zz = lax.rem(z + shift_of(k), NZ)
        for b in range(width // wide):
            columns = slice(b * wide, (b + 1) * wide)
            rows = dot(select[zz], own[:, columns])
            xd[zz, :, :, columns] = rows.reshape(NU, SLP, wide).astype(BF)

        def one(d, _):
            xd_copy(k, d).start()
            return 0

        return lax.fori_loop(1, NU, one, 0)

    lax.fori_loop(0, PACE, send_rows, 0)

    halo_copy.wait_recv()
    keep = jnp.where(flat == 0, 0.0, 1.0)

    def fill_edge(b, _):
        columns = pl.ds(pl.multiple_of(b * 128, 128), 128)
        cpad[b, 0:EDGE, :] = halo[:, columns].astype(F32) * keep
        return 0

    lax.fori_loop(0, blocks, fill_edge, 0)
    convolve(0, EDGE)
    conv_sends[4].start()
    conv_sends[5].start()

    wide_r = lax.broadcasted_iota(jnp.int32, (NU * SLP, CH), 0)
    wide_c = lax.broadcasted_iota(jnp.int32, (NU * SLP, CH), 1)
    spread = ((wide_r & 7) < SL) & (wide_c == (wide_r >> 3) * SL + (wide_r & 7))
    spread = spread.astype(F32).astype(BF)
    pack_r = lax.broadcasted_iota(jnp.int32, (CH, NU * SLP), 0)
    pack_c = lax.broadcasted_iota(jnp.int32, (CH, NU * SLP), 1)
    pack = ((pack_c & 7) < SL) & (pack_r == (pack_c >> 3) * SL + (pack_c & 7))
    pack = pack.astype(F32).astype(BF)

    def disp_copy(k):
        target = lax.rem(z + shift_of(k), NZ)
        return remote(
            disp.at[k], xin.at[k, y], zd_s.at[0], zd_r.at[k], at_zu(target, u), y
        )

    def rows_along(k):
        zz = lax.rem(z + shift_of(k), NZ)

        @pl.when(k < NZ - PACE)
        def _():
            send_rows(k + PACE, 0)

        landed = xdr.at[zz, pl.ds(0, NU - 1)]
        remote(landed, landed, xd_s.at[0], xd_r.at[k], ep, yp).wait_recv()
        xdr[zz, u] = xd[zz, u]

        def narrow(b, _):
            columns = pl.ds(pl.multiple_of(b * wide, wide), wide)
            rows = xdr[zz, :, :, columns].astype(F32).reshape(NU * SLP, wide).astype(BF)
            disp[k, :, columns] = dot(pack, rows).astype(BF)
            return 0

        lax.fori_loop(0, width // wide, narrow, 0, unroll=True)

        @pl.when(k != LOCAL)
        def _():
            disp_copy(k).start()

        @pl.when(k == LOCAL)
        def _():
            xin[k, y] = disp[k]

    def ag_copy(k, n, slot, columns, to):
        where = xin.at[k, slot, :, columns]
        return remote(where, where, ag_s.at[0], ag_r.at[k, n], ep, to)

    def ag_sends(k):
        return [
            ag_copy(k, 0, y, every, yp),
            ag_copy(k, 1, y, every, ym),
            ag_copy(k, 2, ym, low, yp),
            ag_copy(k, 3, yp, high, ym),
        ]

    def rows_out(k):
        @pl.when(k != LOCAL)
        def _():
            disp_copy(k).wait_recv()

        sends = ag_sends(k)
        sends[0].start()
        sends[1].start()

    rows_along(jnp.int32(0))
    rows_along(jnp.int32(1))
    rows_along(jnp.int32(2))
    conv_copy(0, ym, every, yp).wait_recv()
    conv_sends[2].start()
    conv_copy(1, yp, every, ym).wait_recv()
    conv_sends[3].start()
    rows_along(jnp.int32(3))
    rows_out(jnp.int32(0))
    conv_copy(4, ym, every, yp).wait_recv()
    conv_sends[6].start()
    conv_copy(5, yp, every, ym).wait_recv()
    conv_sends[7].start()
    rows_out(jnp.int32(1))
    for load in loads[7:]:
        load.wait()

    def rs_sends(k):
        return [
            remote(part.at[k, yo, :, low], rsa.at[k, 0], rs_s.at[0], rs_r.at[k, 0], ep, yp),
            remote(part.at[k, yo, :, high], rsa.at[k, 1], rs_s.at[0], rs_r.at[k, 1], ep, ym),
            remote(part.at[k, yp], rsb.at[k, 0], rs_s.at[0], rs_r.at[k, 2], ep, yp),
            remote(part.at[k, ym], rsb.at[k, 1], rs_s.at[0], rs_r.at[k, 3], ep, ym),
        ]

    def ret_copy(k, h):
        source = lax.rem(z - shift_of(k) + NZ, NZ)
        columns = (low, high)[h]
        return remote(
            ret.at[k, :, columns],
            back.at[k, :, columns],
            zr_s.at[0],
            zr_r.at[k, h],
            at_zu(source, u),
            y,
        )

    def xr_copy(k, d, columns):
        zz = lax.rem(z + shift_of(k), NZ)
        v = lax.rem(u + d, NU)
        return remote(
            xs.at[k, v, :, columns],
            xr.at[zz, u, :, columns],
            xr_s.at[0],
            xr_r.at[k],
            at_zu(z, v),
            y,
        )

    def rows_on(k):
        sends = ag_sends(k)
        ag_copy(k, 0, ym, every, yp).wait_recv()
        sends[2].start()
        ag_copy(k, 1, yp, every, ym).wait_recv()
        sends[3].start()

    def experts(k):
        ag_copy(k, 2, yo, low, yp).wait_recv()
        ag_copy(k, 3, yo, high, ym).wait_recv()
        rows = xin[k].reshape(NY * CH, width)
        ff = gate.shape[1]
        for b in range(ff // 256):
            columns = slice(b * 256, (b + 1) * 256)
            hid[:, columns] = (silu(dot(rows, gate[:, columns])) * dot(rows, up[:, columns])).astype(BF)

        def project(b, _):
            columns = pl.ds(pl.multiple_of(b * wide, wide), wide)
            out = dot(hid[...], down[:, columns]).astype(BF)
            part[k, :, :, columns] = out.reshape(NY, CH, wide)
            return 0

        lax.fori_loop(0, width // wide, project, 0)
        sends = rs_sends(k)
        sends[0].start()
        sends[1].start()

    def parts_on(k):
        sends = rs_sends(k)
        sends[0].wait_recv()
        kept = part[k, yp, :, low].astype(F32) + rsa[k, 0].astype(F32)
        part[k, yp, :, low] = kept.astype(BF)
        sends[2].start()
        sends[1].wait_recv()
        kept = part[k, ym, :, high].astype(F32) + rsa[k, 1].astype(F32)
        part[k, ym, :, high] = kept.astype(BF)
        sends[3].start()

    def results(k):
        sends = rs_sends(k)
        sends[2].wait_recv()
        sends[3].wait_recv()
        for h, columns in enumerate((low, high)):
            total = part[k, y, :, columns].astype(F32) + rsb[k, 0, :, columns].astype(F32)
            total = (total + rsb[k, 1, :, columns].astype(F32)).astype(BF)

            @pl.when(k != LOCAL)
            def _():
                ret[k, :, columns] = total
                ret_copy(k, h).start()

            @pl.when(k == LOCAL)
            def _():
                back[k, :, columns] = total

    def results_home(k):
        for h, columns in enumerate((low, high)):

            @pl.when(k != LOCAL)
            def _():
                ret_copy(k, h).wait_recv()

            for b in range(half // wide):
                some = pl.ds(h * half + b * wide, wide)
                out = dot(spread, back[k, :, some])
                xs[k, :, :, some] = out.reshape(NU, SLP, wide).astype(BF)

            def send(d, _):
                xr_copy(k, d, columns).start()
                return 0

            lax.fori_loop(1, NU, send, 0)
        xr[lax.rem(z + shift_of(k), NZ), u] = xs[k, u]

    conv_save = pltpu.make_async_copy(conv_held, conv_out, out_sem.at[0])

    def moe_save(b):
        columns = pl.ds(pl.multiple_of(b * wide, wide), wide)
        return pltpu.make_async_copy(moe_held.at[b], moe_out.at[:, columns], out_sem.at[b + 1])

    def beside():
        rows = own[...]
        hidden = (silu(dot(rows, sgate[...])) * dot(rows, sup[...])).astype(BF)
        shared[...] = dot(hidden, sdown[...])
        conv_copy(2, yo, low, yp).wait_recv()
        conv_copy(3, yo, high, ym).wait_recv()
        conv_copy(6, yo, low, yp).wait_recv()
        conv_copy(7, yo, high, ym).wait_recv()

        def project(b, _):
            rows = pl.ds(pl.multiple_of(b * tokens, tokens), tokens)
            conv_held[rows, :] = dot(normed[b], ow[...]).astype(BF)
            return 0

        lax.fori_loop(0, NY, project, 0)
        conv_save.start()

    def stage(i, lag, act):
        k = i - lag

        @pl.when((k >= 0) & (k < NZ))
        def _():
            act(k)

    def step(i, _):
        stage(i, 1, rows_on)

        @pl.when((i >= 2) & (i < NZ))
        def _():
            rows_out(i)

        stage(i, 2, experts)
        stage(i, 3, parts_on)
        stage(i, -EARLY, rows_along)

        @pl.when(i == LOCAL + 4)
        def _():
            results_home(i - HOME)

        stage(i, 4, results)

        @pl.when(i == LOCAL + 4)
        def _():
            results_home(i - 4)

        @pl.when((i >= HOME) & (i != LOCAL + 4))
        def _():
            results_home(i - HOME)

        @pl.when(i == 4)
        def _():
            beside()

        return 0

    lax.fori_loop(0, NZ - 1 + HOME, step, 0)

    def arrived(k, _):
        landed = xr.at[lax.rem(z + shift_of(k), NZ), pl.ds(0, NU - 1)]
        remote(landed, landed, xr_s.at[0], xr_r.at[k], ep, yp).wait_recv()
        return 0

    lax.fori_loop(0, NZ, arrived, 0)

    def combine(b, _):
        columns = pl.ds(pl.multiple_of(b * wide, wide), wide)
        rows = xr[:, :, :, columns].astype(F32).reshape(NZ * NU * SLP, wide).astype(BF)
        both = dot(pick[...], rows)
        routed = both[0:tokens] * weights[:, 0:1] + both[tokens : 2 * tokens] * weights[:, 1:2]
        moe_held[b] = (shared[:, columns] + routed).astype(BF)
        moe_save(b).start()
        return 0

    lax.fori_loop(0, width // wide, combine, 0, unroll=2)

    halo_copy.wait_send()
    sent = pl.ds(0, NU - 1)
    for left, semaphore in (
        (normed.at[pl.ds(0, 3)], cv_s),
        (xd.at[sent], xd_s),
        (disp.at[sent], zd_s),
        (xin.at[:, pl.ds(0, 3)], ag_s),
        (part.at[:, pl.ds(0, 3)], rs_s),
        (ret.at[sent], zr_s),
        (xs.at[sent], xr_s),
    ):
        remote(left, left, semaphore.at[0], halo_sem.at[1], ep, yp).wait_send()
    conv_save.wait()
    for b in range(width // wide):
        moe_save(b).wait()


def hand_on(conv_from, moe_from, conv_to, moe_to, conv_held, moe_held, semaphores):
    copies = [
        pltpu.make_async_copy(source, target, semaphores.at[n])
        for n, (source, target) in enumerate(
            (
                (conv_from, conv_held),
                (moe_from, moe_held),
                (conv_held, conv_to),
                (moe_held, moe_to),
            )
        )
    ]
    copies[0].start()
    copies[1].start()
    copies[0].wait()
    copies[2].start()
    copies[1].wait()
    copies[3].start()
    copies[2].wait()
    copies[3].wait()


def on_device(*args):
    (
        conv_input,
        conv_kernel,
        conv_gain,
        out_weight,
        moe_input,
        moe_gain,
        expert_gate,
        expert_up,
        expert_down,
        shared_gate,
        shared_up,
        shared_down,
        expert_index,
        routing_weight,
    ) = args
    tokens, width = moe_input.shape
    half = width // 2
    ff = expert_gate.shape[2]
    cols = out_weight.shape[1]
    vm = lambda *shape, dtype=BF: pltpu.VMEM(shape, dtype)
    dma = lambda *shape: pltpu.SemaphoreType.DMA(shape)
    in_hbm = pl.BlockSpec(memory_space=pl.ANY)
    operands = (
        (conv_input, in_hbm),
        (conv_kernel, in_hbm),
        (conv_gain.reshape(1, width), in_hbm),
        (out_weight, in_hbm),
        (moe_input, in_hbm),
        (moe_gain.reshape(1, width), in_hbm),
        (expert_gate, in_hbm),
        (expert_up, in_hbm),
        (expert_down, in_hbm),
        (shared_gate, in_hbm),
        (shared_up, in_hbm),
        (shared_down, in_hbm),
        (expert_index.T, in_hbm),
        (routing_weight.T, in_hbm),
    )
    scratch = [
        vm(tokens, width),
        vm(*conv_kernel.shape, dtype=F32),
        vm(1, width, dtype=F32),
        vm(tokens, width),
        vm(1, width, dtype=F32),
        vm(*expert_index.shape[::-1], dtype=jnp.int32),
        vm(*routing_weight.shape[::-1], dtype=F32),
        vm(width, cols),
        vm(width, ff),
        vm(width, ff),
        vm(ff, width),
        vm(*shared_gate.shape),
        vm(*shared_up.shape),
        vm(*shared_down.shape),
        vm(EDGE, width),
        vm(width // 128, EDGE + tokens, 128, dtype=F32),
        vm(tokens, width, dtype=F32),
        vm(NY, tokens, width),
        vm(tokens, width),
        vm(NZ, NU * SLP, tokens),
        vm(NZ, NU, SLP, width),
        vm(NZ, NU, SLP, width),
        vm(NZ, CH, width),
        vm(NZ, NY, CH, width),
        vm(NY * CH, ff),
        vm(NZ, NY, CH, width),
        vm(NZ, 2, CH, half),
        vm(NZ, 2, CH, width),
        vm(NZ, CH, width),
        vm(NZ, CH, width),
        vm(NZ, NU, SLP, width),
        vm(NZ, NU, SLP, width),
        vm(2 * tokens, NZ * NU * SLP),
        vm(tokens, width, dtype=F32),
        vm(tokens, 128, dtype=F32),
        vm(NY * tokens, cols),
        vm(width // 512, tokens, 512),
        dma(14),
        dma(2),
        dma(1),
        dma(NZ),
        dma(1),
        dma(8),
        dma(1),
        dma(NZ),
        dma(1),
        dma(NZ, 4),
        dma(1),
        dma(NZ, 4),
        dma(1),
        dma(NZ, 2),
        dma(1),
        dma(NZ),
        dma(1 + width // 512),
    ]
    shapes = (
        jax.ShapeDtypeStruct((NY * tokens, cols), BF),
        jax.ShapeDtypeStruct((tokens, width), BF),
    )
    results = pl.pallas_call(
        body,
        out_shape=shapes,
        in_specs=[spec for _, spec in operands],
        out_specs=(in_hbm, in_hbm),
        scratch_shapes=scratch,
        compiler_params=pltpu.CompilerParams(
            collective_id=0, has_side_effects=True, vmem_limit_bytes=67043328
        ),
    )(*[array for array, _ in operands])
    return pl.pallas_call(
        hand_on,
        out_shape=shapes,
        in_specs=[in_hbm, in_hbm],
        out_specs=(in_hbm, in_hbm),
        scratch_shapes=[vm(*shape.shape) for shape in shapes] + [dma(4)],
    )(*results)


def solution(mesh):
    in_specs = (
        P(("ep", "tp"), None),
        P(),
        P(),
        P(None, "tp"),
        P(("ep", "tp"), None),
        P(),
        P("ep", None, "tp"),
        P("ep", None, "tp"),
        P("ep", "tp", None),
        P(),
        P(),
        P(),
        P("ep", None),
        P(("ep", "tp"), None),
    )
    out_specs = (P("ep", "tp"), P(("ep", "tp"), None))
    return jax.shard_map(
        on_device, mesh=mesh, in_specs=in_specs, out_specs=out_specs, check_vma=False
    )
```

```python
import functools

import jax
import jax.numpy as jnp
from jax import lax
from jax.experimental import pallas as pl
from jax.experimental.pallas import tpu as pltpu
from jax.sharding import PartitionSpec as P

NORM_EPS = 1e-05
BF = jnp.bfloat16
F32 = jnp.float32
MESH_ID = pl.DeviceIdType.MESH
NZ, NU, NY = 8, 8, 4
SL = 6
SLP = 8
CH = NU * SL
ROWS = 16
EDGE = 32
HOME = 6
PACE = 3
EARLY = 4


def remote(src, dst, send, recv, ep, tp):
    return pltpu.make_async_remote_copy(
        src_ref=src,
        dst_ref=dst,
        send_sem=send,
        recv_sem=recv,
        device_id=(ep, tp),
        device_id_type=MESH_ID,
    )


ORDER = (0, 6, 3, 5, 4, 2, 7, 1)
LOCAL = ORDER.index(0)
PACKED = sum(far << (4 * k) for k, far in enumerate(ORDER))


def shift_of(k):
    return lax.shift_right_logical(jnp.int32(PACKED), jnp.int32(4) * k) & 7


def silu(a):
    return a * lax.logistic(a)


def scaled(values, gain):
    center = values - jnp.mean(values, axis=-1, keepdims=True)
    spread = jnp.mean(center * center, axis=-1, keepdims=True)
    return center * lax.rsqrt(spread + NORM_EPS) * gain


def dot(a, b):
    return jnp.dot(a, b, preferred_element_type=F32)


def body(
    conv_hbm,
    taps_hbm,
    conv_g_hbm,
    ow_hbm,
    moe_hbm,
    moe_g_hbm,
    gate_hbm,
    up_hbm,
    down_hbm,
    sgate_hbm,
    sup_hbm,
    sdown_hbm,
    index_hbm,
    weight_hbm,
    conv_out,
    moe_out,
    conv_in,
    conv_k,
    conv_g,
    moe_in,
    moe_g,
    index,
    weight,
    ow,
    gate,
    up,
    down,
    sgate,
    sup,
    sdown,
    halo,
    cpad,
    mixed,
    normed,
    own,
    select,
    xd,
    xdr,
    disp,
    xin,
    hid,
    part,
    rsa,
    rsb,
    ret,
    back,
    xs,
    xr,
    pick,
    shared,
    weights,
    conv_held,
    moe_held,
    ld,
    halo_sem,
    xd_s,
    xd_r,
    cv_s,
    cv_r,
    zd_s,
    zd_r,
    ag_s,
    ag_r,
    rs_s,
    rs_r,
    zr_s,
    zr_r,
    xr_s,
    xr_r,
    out_sem,
):
    tokens, width = moe_in.shape
    half = width // 2
    wide = 512
    every, low, high = pl.ds(0, width), pl.ds(0, half), pl.ds(half, half)
    ep = lax.axis_index("ep")
    y = lax.axis_index("tp")
    z, u = lax.div(ep, NU), lax.rem(ep, NU)
    yp, ym, yo = lax.rem(y + 1, NY), lax.rem(y + NY - 1, NY), lax.rem(y + 2, NY)

    def at_zu(zz, uu):
        return zz * NU + uu

    flat = ep * NY + y
    count = NZ * NU * NY
    ahead = lax.rem(flat + 1, count)
    behind = lax.rem(flat + count - 1, count)

    barrier = pltpu.get_barrier_semaphore()

    def greet(e, t):
        pl.semaphore_signal(barrier, inc=1, device_id=(e, t), device_id_type=MESH_ID)

    greet(ep, yp)
    greet(ep, ym)
    for d in range(1, NZ):
        greet(at_zu(lax.rem(z + d, NZ), u), y)
    for d in range(1, NU):
        greet(at_zu(z, lax.rem(u + d, NU)), y)
    greet(lax.div(ahead, NY), lax.rem(ahead, NY))
    greet(lax.div(behind, NY), lax.rem(behind, NY))

    loads = [
        pltpu.make_async_copy(source, target, ld.at[n])
        for n, (source, target) in enumerate(
            (
                (conv_hbm, conv_in),
                (taps_hbm, conv_k),
                (conv_g_hbm, conv_g),
                (index_hbm, index),
                (weight_hbm, weight),
                (moe_hbm, moe_in),
                (moe_g_hbm, moe_g),
                (gate_hbm.at[0], gate),
                (up_hbm.at[0], up),
                (down_hbm.at[0], down),
                (ow_hbm, ow),
                (sgate_hbm, sgate),
                (sup_hbm, sup),
                (sdown_hbm, sdown),
            )
        )
    ]
    for load in loads:
        load.start()

    blocks = width // 128
    taps = conv_k.shape[0]
    for load in loads[0:3]:
        load.wait()

    def fill(b, _):
        columns = pl.ds(pl.multiple_of(b * 128, 128), 128)
        cpad[b, EDGE : EDGE + tokens, :] = conv_in[:, columns].astype(F32)
        return 0

    lax.fori_loop(0, blocks, fill, 0)

    def convolve(begin, length):
        def one(b, _):
            columns = pl.ds(pl.multiple_of(b * 128, 128), 128)
            total = jnp.zeros((length, 128), F32)
            for k in range(taps):
                start = begin + EDGE + 1 - taps + k
                total = total + cpad[b, start : start + length, :] * conv_k[k : k + 1, columns]
            mixed[begin : begin + length, columns] = total
            return 0

        lax.fori_loop(0, blocks, one, 0)

        def conv_norm(r, _):
            rows = pl.ds(pl.multiple_of(begin + r * ROWS, ROWS), ROWS)
            normed[y, rows, :] = silu(scaled(mixed[rows, :], conv_g[...])).astype(BF)
            return 0

        lax.fori_loop(0, length // ROWS, conv_norm, 0, unroll=2)

    def conv_copy(n, slot, columns, to):
        rows = pl.ds(EDGE, tokens - EDGE) if n < 4 else pl.ds(0, EDGE)
        where = normed.at[slot, rows, columns]
        return remote(where, where, cv_s.at[0], cv_r.at[n], ep, to)

    conv_sends = [
        conv_copy(0, y, every, yp),
        conv_copy(1, y, every, ym),
        conv_copy(2, ym, low, yp),
        conv_copy(3, yp, high, ym),
        conv_copy(4, y, every, yp),
        conv_copy(5, y, every, ym),
        conv_copy(6, ym, low, yp),
        conv_copy(7, yp, high, ym),
    ]
    convolve(EDGE, tokens - EDGE)

    pl.semaphore_wait(barrier, NZ - 1 + NU - 1 + 4)

    halo_copy = remote(
        conv_in.at[pl.ds(tokens - EDGE, EDGE), :],
        halo,
        halo_sem.at[0],
        halo_sem.at[1],
        lax.div(ahead, NY),
        lax.rem(ahead, NY),
    )
    halo_copy.start()
    conv_sends[0].start()
    conv_sends[1].start()

    loads[3].wait()
    loads[4].wait()

    mine = index[:, pl.ds(pl.multiple_of(y * tokens, tokens), tokens)]
    expert = lax.broadcasted_iota(jnp.int32, (NZ * NU, tokens), 0)
    first = expert == mine[0:1, :]
    second = expert == mine[1:2, :]
    named = (first | second).astype(F32).astype(BF)
    row_i = lax.broadcasted_iota(jnp.int32, (tokens, tokens), 0)
    col_i = lax.broadcasted_iota(jnp.int32, (tokens, tokens), 1)
    rank = dot(named, (row_i < col_i).astype(F32).astype(BF))
    rank_first = jnp.sum(jnp.where(first, rank, 0.0), axis=0, keepdims=True)
    rank_second = jnp.sum(jnp.where(second, rank, 0.0), axis=0, keepdims=True)
    place_first = mine[0:1, :] * SLP + rank_first.astype(jnp.int32)
    place_second = mine[1:2, :] * SLP + rank_second.astype(jnp.int32)
    place = lax.broadcasted_iota(jnp.int32, (NZ * NU * SLP, tokens), 0)
    hits = ((place == place_first) | (place == place_second)).astype(F32).astype(BF)
    select[...] = hits.reshape(NZ, NU * SLP, tokens)

    share = weight[...]
    share_a = share.astype(BF).astype(F32)
    share_b = (share - share_a).astype(BF).astype(F32)
    share_c = share - share_a - share_b
    line = lax.broadcasted_iota(jnp.int32, (16, tokens), 0)
    table = jnp.zeros((16, tokens), F32)
    for n, values in enumerate(
        (
            mine[0:1, :].astype(F32),
            mine[1:2, :].astype(F32),
            rank_first,
            rank_second,
            share_a[0:1, :],
            share_a[1:2, :],
            share_b[0:1, :],
            share_b[1:2, :],
            share_c[0:1, :],
            share_c[1:2, :],
        )
    ):
        table = jnp.where(line == n, values, table)
    turned = lax.dot_general(
        (row_i == col_i).astype(F32).astype(BF),
        table.astype(BF),
        (((1,), (1,)), ((), ())),
        preferred_element_type=F32,
    )
    weights[:, 0:2] = turned[:, 4:6] + turned[:, 6:8] + turned[:, 8:10]
    places = (turned[:, 0:2] * SLP + turned[:, 2:4]).astype(jnp.int32)
    spot = lax.broadcasted_iota(jnp.int32, (tokens, NZ * NU * SLP), 1)
    pick[0:tokens, :] = (spot == places[:, 0:1]).astype(F32).astype(BF)
    pick[tokens : 2 * tokens, :] = (spot == places[:, 1:2]).astype(F32).astype(BF)

    loads[5].wait()
    loads[6].wait()

    def norm_rows(r, _):
        rows = pl.ds(pl.multiple_of(r * ROWS, ROWS), ROWS)
        own[rows, :] = scaled(moe_in[rows, :].astype(F32), moe_g[...]).astype(BF)
        return 0

    lax.fori_loop(0, tokens // ROWS, norm_rows, 0, unroll=4)

    def xd_copy(k, d):
        zz = lax.rem(z + shift_of(k), NZ)
        v = lax.rem(u + d, NU)
        return remote(
            xd.at[zz, v], xdr.at[zz, u], xd_s.at[0], xd_r.at[k], at_zu(z, v), y
        )

    def send_rows(k, _):
        zz = lax.rem(z + shift_of(k), NZ)
        for b in range(width // wide):
            columns = slice(b * wide, (b + 1) * wide)
            rows = dot(select[zz], own[:, columns])
            xd[zz, :, :, columns] = rows.reshape(NU, SLP, wide).astype(BF)

        def one(d, _):
            xd_copy(k, d).start()
            return 0

        return lax.fori_loop(1, NU, one, 0)

    lax.fori_loop(0, PACE, send_rows, 0)

    halo_copy.wait_recv()
    keep = jnp.where(flat == 0, 0.0, 1.0)

    def fill_edge(b, _):
        columns = pl.ds(pl.multiple_of(b * 128, 128), 128)
        cpad[b, 0:EDGE, :] = halo[:, columns].astype(F32) * keep
        return 0

    lax.fori_loop(0, blocks, fill_edge, 0)
    convolve(0, EDGE)
    conv_sends[4].start()
    conv_sends[5].start()

    wide_r = lax.broadcasted_iota(jnp.int32, (NU * SLP, CH), 0)
    wide_c = lax.broadcasted_iota(jnp.int32, (NU * SLP, CH), 1)
    spread = ((wide_r & 7) < SL) & (wide_c == (wide_r >> 3) * SL + (wide_r & 7))
    spread = spread.astype(F32).astype(BF)
    pack_r = lax.broadcasted_iota(jnp.int32, (CH, NU * SLP), 0)
    pack_c = lax.broadcasted_iota(jnp.int32, (CH, NU * SLP), 1)
    pack = ((pack_c & 7) < SL) & (pack_r == (pack_c >> 3) * SL + (pack_c & 7))
    pack = pack.astype(F32).astype(BF)

    def disp_copy(k):
        target = lax.rem(z + shift_of(k), NZ)
        return remote(
            disp.at[k], xin.at[k, y], zd_s.at[0], zd_r.at[k], at_zu(target, u), y
        )

    def rows_along(k):
        zz = lax.rem(z + shift_of(k), NZ)

        @pl.when(k < NZ - PACE)
        def _():
            send_rows(k + PACE, 0)

        landed = xdr.at[zz, pl.ds(0, NU - 1)]
        remote(landed, landed, xd_s.at[0], xd_r.at[k], ep, yp).wait_recv()
        xdr[zz, u] = xd[zz, u]

        def narrow(b, _):
            columns = pl.ds(pl.multiple_of(b * wide, wide), wide)
            rows = xdr[zz, :, :, columns].astype(F32).reshape(NU * SLP, wide).astype(BF)
            disp[k, :, columns] = dot(pack, rows).astype(BF)
            return 0

        lax.fori_loop(0, width // wide, narrow, 0, unroll=True)

        @pl.when(k != LOCAL)
        def _():
            disp_copy(k).start()

        @pl.when(k == LOCAL)
        def _():
            xin[k, y] = disp[k]

    def ag_copy(k, n, slot, columns, to):
        where = xin.at[k, slot, :, columns]
        return remote(where, where, ag_s.at[0], ag_r.at[k, n], ep, to)

    def ag_sends(k):
        return [
            ag_copy(k, 0, y, every, yp),
            ag_copy(k, 1, y, every, ym),
            ag_copy(k, 2, ym, low, yp),
            ag_copy(k, 3, yp, high, ym),
        ]

    def rows_out(k):
        @pl.when(k != LOCAL)
        def _():
            disp_copy(k).wait_recv()

        sends = ag_sends(k)
        sends[0].start()
        sends[1].start()

    rows_along(jnp.int32(0))
    rows_out(jnp.int32(0))
    for k in range(1, EARLY):
        rows_along(jnp.int32(k))
    for load in loads[7:]:
        load.wait()

    def rs_sends(k):
        return [
            remote(part.at[k, yo, :, low], rsa.at[k, 0], rs_s.at[0], rs_r.at[k, 0], ep, yp),
            remote(part.at[k, yo, :, high], rsa.at[k, 1], rs_s.at[0], rs_r.at[k, 1], ep, ym),
            remote(part.at[k, yp], rsb.at[k, 0], rs_s.at[0], rs_r.at[k, 2], ep, yp),
            remote(part.at[k, ym], rsb.at[k, 1], rs_s.at[0], rs_r.at[k, 3], ep, ym),
        ]

    def ret_copy(k, h):
        source = lax.rem(z - shift_of(k) + NZ, NZ)
        columns = (low, high)[h]
        return remote(
            ret.at[k, :, columns],
            back.at[k, :, columns],
            zr_s.at[0],
            zr_r.at[k, h],
            at_zu(source, u),
            y,
        )

    def xr_copy(k, d, columns):
        zz = lax.rem(z + shift_of(k), NZ)
        v = lax.rem(u + d, NU)
        return remote(
            xs.at[k, v, :, columns],
            xr.at[zz, u, :, columns],
            xr_s.at[0],
            xr_r.at[k],
            at_zu(z, v),
            y,
        )

    def rows_on(k):
        sends = ag_sends(k)
        ag_copy(k, 0, ym, every, yp).wait_recv()
        sends[2].start()
        ag_copy(k, 1, yp, every, ym).wait_recv()
        sends[3].start()

    def experts(k):
        ag_copy(k, 2, yo, low, yp).wait_recv()
        ag_copy(k, 3, yo, high, ym).wait_recv()
        rows = xin[k].reshape(NY * CH, width)
        ff = gate.shape[1]
        for b in range(ff // 256):
            columns = slice(b * 256, (b + 1) * 256)
            hid[:, columns] = (silu(dot(rows, gate[:, columns])) * dot(rows, up[:, columns])).astype(BF)

        def project(b, _):
            columns = pl.ds(pl.multiple_of(b * wide, wide), wide)
            out = dot(hid[...], down[:, columns]).astype(BF)
            part[k, :, :, columns] = out.reshape(NY, CH, wide)
            return 0

        lax.fori_loop(0, width // wide, project, 0)
        sends = rs_sends(k)
        sends[0].start()
        sends[1].start()

    def parts_on(k):
        sends = rs_sends(k)
        sends[0].wait_recv()
        kept = part[k, yp, :, low].astype(F32) + rsa[k, 0].astype(F32)
        part[k, yp, :, low] = kept.astype(BF)
        sends[2].start()
        sends[1].wait_recv()
        kept = part[k, ym, :, high].astype(F32) + rsa[k, 1].astype(F32)
        part[k, ym, :, high] = kept.astype(BF)
        sends[3].start()

    def results(k):
        sends = rs_sends(k)
        sends[2].wait_recv()
        sends[3].wait_recv()
        for h, columns in enumerate((low, high)):
            total = part[k, y, :, columns].astype(F32) + rsb[k, 0, :, columns].astype(F32)
            total = (total + rsb[k, 1, :, columns].astype(F32)).astype(BF)

            @pl.when(k != LOCAL)
            def _():
                ret[k, :, columns] = total
                ret_copy(k, h).start()

            @pl.when(k == LOCAL)
            def _():
                back[k, :, columns] = total

    def results_home(k):
        for h, columns in enumerate((low, high)):

            @pl.when(k != LOCAL)
            def _():
                ret_copy(k, h).wait_recv()

            for b in range(half // wide):
                some = pl.ds(h * half + b * wide, wide)
                out = dot(spread, back[k, :, some])
                xs[k, :, :, some] = out.reshape(NU, SLP, wide).astype(BF)

            def send(d, _):
                xr_copy(k, d, columns).start()
                return 0

            lax.fori_loop(1, NU, send, 0)
        xr[lax.rem(z + shift_of(k), NZ), u] = xs[k, u]

    conv_save = pltpu.make_async_copy(conv_held, conv_out, out_sem.at[0])

    def moe_save(b):
        columns = pl.ds(pl.multiple_of(b * wide, wide), wide)
        return pltpu.make_async_copy(moe_held.at[b], moe_out.at[:, columns], out_sem.at[b + 1])

    def beside():
        rows = own[...]
        hidden = (silu(dot(rows, sgate[...])) * dot(rows, sup[...])).astype(BF)
        shared[...] = dot(hidden, sdown[...])
        for n, slot in enumerate((ym, yp)):
            conv_copy(n, slot, every, yp).wait_recv()
            conv_copy(n + 4, slot, every, yp).wait_recv()

        def project(n, _):
            conv_project(lax.rem(y + NY - 1 + n, NY))
            return 0

        lax.fori_loop(0, 3, project, 0)

    def conv_project(b):
        rows = pl.ds(pl.multiple_of(b * tokens, tokens), tokens)
        conv_held[rows, :] = dot(normed[b], ow[...]).astype(BF)

    def conv_forward():
        for n in (2, 3, 6, 7):
            conv_sends[n].start()

    def conv_last():
        for n in (2, 6):
            conv_copy(n, yo, low, yp).wait_recv()
            conv_copy(n + 1, yo, high, ym).wait_recv()
        conv_project(yo)
        conv_save.start()

    def stage(i, lag, act):
        k = i - lag

        @pl.when((k >= 0) & (k < NZ))
        def _():
            act(k)

    def step(i, _):
        stage(i, 1, rows_on)

        @pl.when((i >= 1) & (i < NZ))
        def _():
            rows_out(i)

        stage(i, 2, experts)
        stage(i, 3, parts_on)

        @pl.when(i == NZ + 2)
        def _():
            conv_forward()

        stage(i, -EARLY, rows_along)
        stage(i, 4, results)
        stage(i, HOME, results_home)

        @pl.when(i == 4)
        def _():
            beside()

        return 0

    lax.fori_loop(0, NZ + HOME, step, 0)
    conv_last()

    def arrived(k, _):
        landed = xr.at[lax.rem(z + shift_of(k), NZ), pl.ds(0, NU - 1)]
        remote(landed, landed, xr_s.at[0], xr_r.at[k], ep, yp).wait_recv()
        return 0

    lax.fori_loop(0, NZ, arrived, 0)

    def combine(b, _):
        columns = pl.ds(pl.multiple_of(b * wide, wide), wide)
        rows = xr[:, :, :, columns].astype(F32).reshape(NZ * NU * SLP, wide).astype(BF)
        both = dot(pick[...], rows)
        routed = both[0:tokens] * weights[:, 0:1] + both[tokens : 2 * tokens] * weights[:, 1:2]
        moe_held[b] = (shared[:, columns] + routed).astype(BF)
        moe_save(b).start()
        return 0

    lax.fori_loop(0, width // wide, combine, 0, unroll=2)

    halo_copy.wait_send()
    sent = pl.ds(0, NU - 1)
    for left, semaphore in (
        (normed.at[pl.ds(0, 3)], cv_s),
        (xd.at[sent], xd_s),
        (disp.at[sent], zd_s),
        (xin.at[:, pl.ds(0, 3)], ag_s),
        (part.at[:, pl.ds(0, 3)], rs_s),
        (ret.at[sent], zr_s),
        (xs.at[sent], xr_s),
    ):
        remote(left, left, semaphore.at[0], halo_sem.at[1], ep, yp).wait_send()
    conv_save.wait()
    for b in range(width // wide):
        moe_save(b).wait()


def hand_on(conv_from, moe_from, conv_to, moe_to, conv_held, moe_held, semaphores):
    copies = [
        pltpu.make_async_copy(source, target, semaphores.at[n])
        for n, (source, target) in enumerate(
            (
                (conv_from, conv_held),
                (moe_from, moe_held),
                (conv_held, conv_to),
                (moe_held, moe_to),
            )
        )
    ]
    copies[0].start()
    copies[1].start()
    copies[0].wait()
    copies[2].start()
    copies[1].wait()
    copies[3].start()
    copies[2].wait()
    copies[3].wait()


def on_device(*args):
    (
        conv_input,
        conv_kernel,
        conv_gain,
        out_weight,
        moe_input,
        moe_gain,
        expert_gate,
        expert_up,
        expert_down,
        shared_gate,
        shared_up,
        shared_down,
        expert_index,
        routing_weight,
    ) = args
    tokens, width = moe_input.shape
    half = width // 2
    ff = expert_gate.shape[2]
    cols = out_weight.shape[1]
    vm = lambda *shape, dtype=BF: pltpu.VMEM(shape, dtype)
    dma = lambda *shape: pltpu.SemaphoreType.DMA(shape)
    in_hbm = pl.BlockSpec(memory_space=pl.ANY)
    operands = (
        (conv_input, in_hbm),
        (conv_kernel, in_hbm),
        (conv_gain.reshape(1, width), in_hbm),
        (out_weight, in_hbm),
        (moe_input, in_hbm),
        (moe_gain.reshape(1, width), in_hbm),
        (expert_gate, in_hbm),
        (expert_up, in_hbm),
        (expert_down, in_hbm),
        (shared_gate, in_hbm),
        (shared_up, in_hbm),
        (shared_down, in_hbm),
        (expert_index.T, in_hbm),
        (routing_weight.T, in_hbm),
    )
    scratch = [
        vm(tokens, width),
        vm(*conv_kernel.shape, dtype=F32),
        vm(1, width, dtype=F32),
        vm(tokens, width),
        vm(1, width, dtype=F32),
        vm(*expert_index.shape[::-1], dtype=jnp.int32),
        vm(*routing_weight.shape[::-1], dtype=F32),
        vm(width, cols),
        vm(width, ff),
        vm(width, ff),
        vm(ff, width),
        vm(*shared_gate.shape),
        vm(*shared_up.shape),
        vm(*shared_down.shape),
        vm(EDGE, width),
        vm(width // 128, EDGE + tokens, 128, dtype=F32),
        vm(tokens, width, dtype=F32),
        vm(NY, tokens, width),
        vm(tokens, width),
        vm(NZ, NU * SLP, tokens),
        vm(NZ, NU, SLP, width),
        vm(NZ, NU, SLP, width),
        vm(NZ, CH, width),
        vm(NZ, NY, CH, width),
        vm(NY * CH, ff),
        vm(NZ, NY, CH, width),
        vm(NZ, 2, CH, half),
        vm(NZ, 2, CH, width),
        vm(NZ, CH, width),
        vm(NZ, CH, width),
        vm(NZ, NU, SLP, width),
        vm(NZ, NU, SLP, width),
        vm(2 * tokens, NZ * NU * SLP),
        vm(tokens, width, dtype=F32),
        vm(tokens, 128, dtype=F32),
        vm(NY * tokens, cols),
        vm(width // 512, tokens, 512),
        dma(14),
        dma(2),
        dma(1),
        dma(NZ),
        dma(1),
        dma(8),
        dma(1),
        dma(NZ),
        dma(1),
        dma(NZ, 4),
        dma(1),
        dma(NZ, 4),
        dma(1),
        dma(NZ, 2),
        dma(1),
        dma(NZ),
        dma(1 + width // 512),
    ]
    shapes = (
        jax.ShapeDtypeStruct((NY * tokens, cols), BF),
        jax.ShapeDtypeStruct((tokens, width), BF),
    )
    results = pl.pallas_call(
        body,
        out_shape=shapes,
        in_specs=[spec for _, spec in operands],
        out_specs=(in_hbm, in_hbm),
        scratch_shapes=scratch,
        compiler_params=pltpu.CompilerParams(
            collective_id=0, has_side_effects=True, vmem_limit_bytes=67043328
        ),
    )(*[array for array, _ in operands])
    return pl.pallas_call(
        hand_on,
        out_shape=shapes,
        in_specs=[in_hbm, in_hbm],
        out_specs=(in_hbm, in_hbm),
        scratch_shapes=[vm(*shape.shape) for shape in shapes] + [dma(4)],
    )(*results)


def solution(mesh):
    in_specs = (
        P(("ep", "tp"), None),
        P(),
        P(),
        P(None, "tp"),
        P(("ep", "tp"), None),
        P(),
        P("ep", None, "tp"),
        P("ep", None, "tp"),
        P("ep", "tp", None),
        P(),
        P(),
        P(),
        P("ep", None),
        P(("ep", "tp"), None),
    )
    out_specs = (P("ep", "tp"), P(("ep", "tp"), None))
    return jax.shard_map(
        on_device, mesh=mesh, in_specs=in_specs, out_specs=out_specs, check_vma=False
    )
```

```python
import functools

import jax
import jax.numpy as jnp
from jax import lax
from jax.experimental import pallas as pl
from jax.experimental.pallas import tpu as pltpu
from jax.sharding import PartitionSpec as P

NORM_EPS = 1e-05
BF = jnp.bfloat16
F32 = jnp.float32
MESH_ID = pl.DeviceIdType.MESH
NZ, NU, NY = 8, 8, 4
SL = 6
SLP = 8
CH = NU * SL
ROWS = 16
EDGE = 32
HOME = 6
PACE = 3
EARLY = 4


def remote(src, dst, send, recv, ep, tp):
    return pltpu.make_async_remote_copy(
        src_ref=src,
        dst_ref=dst,
        send_sem=send,
        recv_sem=recv,
        device_id=(ep, tp),
        device_id_type=MESH_ID,
    )


ORDER = (0, 6, 3, 5, 4, 2, 7, 1)
LOCAL = ORDER.index(0)
PACKED = sum(far << (4 * k) for k, far in enumerate(ORDER))


def shift_of(k):
    return lax.shift_right_logical(jnp.int32(PACKED), jnp.int32(4) * k) & 7


def silu(a):
    return a * lax.logistic(a)


def scaled(values, gain):
    center = values - jnp.mean(values, axis=-1, keepdims=True)
    spread = jnp.mean(center * center, axis=-1, keepdims=True)
    return center * lax.rsqrt(spread + NORM_EPS) * gain


def dot(a, b):
    return jnp.dot(a, b, preferred_element_type=F32)


def body(
    conv_hbm,
    taps_hbm,
    conv_g_hbm,
    ow_hbm,
    moe_hbm,
    moe_g_hbm,
    gate_hbm,
    up_hbm,
    down_hbm,
    sgate_hbm,
    sup_hbm,
    sdown_hbm,
    index_hbm,
    weight_hbm,
    conv_out,
    moe_out,
    conv_in,
    conv_k,
    conv_g,
    moe_in,
    moe_g,
    index,
    weight,
    ow,
    gate,
    up,
    down,
    sgate,
    sup,
    sdown,
    halo,
    cpad,
    mixed,
    normed,
    own,
    select,
    xd,
    xdr,
    disp,
    xin,
    hid,
    part,
    rsa,
    rsb,
    ret,
    back,
    xs,
    xr,
    pick,
    shared,
    weights,
    ld,
    halo_sem,
    xd_s,
    xd_r,
    cv_s,
    cv_r,
    zd_s,
    zd_r,
    ag_s,
    ag_r,
    rs_s,
    rs_r,
    zr_s,
    zr_r,
    xr_s,
    xr_r,
):
    tokens, width = moe_in.shape
    half = width // 2
    wide = 512
    every, low, high = pl.ds(0, width), pl.ds(0, half), pl.ds(half, half)
    ep = lax.axis_index("ep")
    y = lax.axis_index("tp")
    z, u = lax.div(ep, NU), lax.rem(ep, NU)
    yp, ym, yo = lax.rem(y + 1, NY), lax.rem(y + NY - 1, NY), lax.rem(y + 2, NY)

    def at_zu(zz, uu):
        return zz * NU + uu

    flat = ep * NY + y
    count = NZ * NU * NY
    ahead = lax.rem(flat + 1, count)
    behind = lax.rem(flat + count - 1, count)

    barrier = pltpu.get_barrier_semaphore()

    def greet(e, t):
        pl.semaphore_signal(barrier, inc=1, device_id=(e, t), device_id_type=MESH_ID)

    greet(ep, yp)
    greet(ep, ym)
    for d in range(1, NZ):
        greet(at_zu(lax.rem(z + d, NZ), u), y)
    for d in range(1, NU):
        greet(at_zu(z, lax.rem(u + d, NU)), y)
    greet(lax.div(ahead, NY), lax.rem(ahead, NY))
    greet(lax.div(behind, NY), lax.rem(behind, NY))

    loads = [
        pltpu.make_async_copy(source, target, ld.at[n])
        for n, (source, target) in enumerate(
            (
                (conv_hbm, conv_in),
                (taps_hbm, conv_k),
                (conv_g_hbm, conv_g),
                (index_hbm, index),
                (weight_hbm, weight),
                (moe_hbm, moe_in),
                (moe_g_hbm, moe_g),
                (gate_hbm.at[0], gate),
                (up_hbm.at[0], up),
                (down_hbm.at[0], down),
                (ow_hbm, ow),
                (sgate_hbm, sgate),
                (sup_hbm, sup),
                (sdown_hbm, sdown),
            )
        )
    ]
    for load in loads:
        load.start()

    blocks = width // 128
    taps = conv_k.shape[0]
    for load in loads[0:3]:
        load.wait()

    def fill(b, _):
        columns = pl.ds(pl.multiple_of(b * 128, 128), 128)
        cpad[b, EDGE : EDGE + tokens, :] = conv_in[:, columns].astype(F32)
        return 0

    lax.fori_loop(0, blocks, fill, 0)

    def convolve(begin, length):
        def one(b, _):
            columns = pl.ds(pl.multiple_of(b * 128, 128), 128)
            total = jnp.zeros((length, 128), F32)
            for k in range(taps):
                start = begin + EDGE + 1 - taps + k
                total = total + cpad[b, start : start + length, :] * conv_k[k : k + 1, columns]
            mixed[begin : begin + length, columns] = total
            return 0

        lax.fori_loop(0, blocks, one, 0)

        def conv_norm(r, _):
            rows = pl.ds(pl.multiple_of(begin + r * ROWS, ROWS), ROWS)
            normed[y, rows, :] = silu(scaled(mixed[rows, :], conv_g[...])).astype(BF)
            return 0

        lax.fori_loop(0, length // ROWS, conv_norm, 0, unroll=2)

    def conv_copy(n, slot, columns, to):
        rows = pl.ds(EDGE, tokens - EDGE) if n < 4 else pl.ds(0, EDGE)
        where = normed.at[slot, rows, columns]
        return remote(where, where, cv_s.at[0], cv_r.at[n], ep, to)

    conv_sends = [
        conv_copy(0, y, every, yp),
        conv_copy(1, y, every, ym),
        conv_copy(2, ym, low, yp),
        conv_copy(3, yp, high, ym),
        conv_copy(4, y, every, yp),
        conv_copy(5, y, every, ym),
        conv_copy(6, ym, low, yp),
        conv_copy(7, yp, high, ym),
    ]
    convolve(EDGE, tokens - EDGE)

    pl.semaphore_wait(barrier, NZ - 1 + NU - 1 + 4)

    halo_copy = remote(
        conv_in.at[pl.ds(tokens - EDGE, EDGE), :],
        halo,
        halo_sem.at[0],
        halo_sem.at[1],
        lax.div(ahead, NY),
        lax.rem(ahead, NY),
    )
    halo_copy.start()
    conv_sends[0].start()
    conv_sends[1].start()

    loads[3].wait()
    loads[4].wait()

    mine = index[:, pl.ds(pl.multiple_of(y * tokens, tokens), tokens)]
    expert = lax.broadcasted_iota(jnp.int32, (NZ * NU, tokens), 0)
    first = expert == mine[0:1, :]
    second = expert == mine[1:2, :]
    named = (first | second).astype(F32).astype(BF)
    row_i = lax.broadcasted_iota(jnp.int32, (tokens, tokens), 0)
    col_i = lax.broadcasted_iota(jnp.int32, (tokens, tokens), 1)
    rank = dot(named, (row_i < col_i).astype(F32).astype(BF))
    rank_first = jnp.sum(jnp.where(first, rank, 0.0), axis=0, keepdims=True)
    rank_second = jnp.sum(jnp.where(second, rank, 0.0), axis=0, keepdims=True)
    place_first = mine[0:1, :] * SLP + rank_first.astype(jnp.int32)
    place_second = mine[1:2, :] * SLP + rank_second.astype(jnp.int32)
    place = lax.broadcasted_iota(jnp.int32, (NZ * NU * SLP, tokens), 0)
    hits = ((place == place_first) | (place == place_second)).astype(F32).astype(BF)
    select[...] = hits.reshape(NZ, NU * SLP, tokens)

    share = weight[...]
    share_a = share.astype(BF).astype(F32)
    share_b = (share - share_a).astype(BF).astype(F32)
    share_c = share - share_a - share_b
    line = lax.broadcasted_iota(jnp.int32, (16, tokens), 0)
    table = jnp.zeros((16, tokens), F32)
    for n, values in enumerate(
        (
            mine[0:1, :].astype(F32),
            mine[1:2, :].astype(F32),
            rank_first,
            rank_second,
            share_a[0:1, :],
            share_a[1:2, :],
            share_b[0:1, :],
            share_b[1:2, :],
            share_c[0:1, :],
            share_c[1:2, :],
        )
    ):
        table = jnp.where(line == n, values, table)
    turned = lax.dot_general(
        (row_i == col_i).astype(F32).astype(BF),
        table.astype(BF),
        (((1,), (1,)), ((), ())),
        preferred_element_type=F32,
    )
    weights[:, 0:2] = turned[:, 4:6] + turned[:, 6:8] + turned[:, 8:10]
    places = (turned[:, 0:2] * SLP + turned[:, 2:4]).astype(jnp.int32)
    spot = lax.broadcasted_iota(jnp.int32, (tokens, NZ * NU * SLP), 1)
    pick[0:tokens, :] = (spot == places[:, 0:1]).astype(F32).astype(BF)
    pick[tokens : 2 * tokens, :] = (spot == places[:, 1:2]).astype(F32).astype(BF)

    loads[5].wait()
    loads[6].wait()

    def norm_rows(r, _):
        rows = pl.ds(pl.multiple_of(r * ROWS, ROWS), ROWS)
        own[rows, :] = scaled(moe_in[rows, :].astype(F32), moe_g[...]).astype(BF)
        return 0

    lax.fori_loop(0, tokens // ROWS, norm_rows, 0, unroll=4)

    def xd_copy(k, d):
        zz = lax.rem(z + shift_of(k), NZ)
        v = lax.rem(u + d, NU)
        return remote(
            xd.at[zz, v], xdr.at[zz, u], xd_s.at[0], xd_r.at[k], at_zu(z, v), y
        )

    def send_rows(k, _):
        zz = lax.rem(z + shift_of(k), NZ)
        for b in range(width // wide):
            columns = slice(b * wide, (b + 1) * wide)
            rows = dot(select[zz], own[:, columns])
            xd[zz, :, :, columns] = rows.reshape(NU, SLP, wide).astype(BF)

        def one(d, _):
            xd_copy(k, d).start()
            return 0

        return lax.fori_loop(1, NU, one, 0)

    send_rows(jnp.int32(1), 0)
    send_rows(jnp.int32(0), 0)
    send_rows(jnp.int32(2), 0)

    halo_copy.wait_recv()
    keep = jnp.where(flat == 0, 0.0, 1.0)

    def fill_edge(b, _):
        columns = pl.ds(pl.multiple_of(b * 128, 128), 128)
        cpad[b, 0:EDGE, :] = halo[:, columns].astype(F32) * keep
        return 0

    lax.fori_loop(0, blocks, fill_edge, 0)
    convolve(0, EDGE)
    conv_sends[4].start()
    conv_sends[5].start()

    wide_r = lax.broadcasted_iota(jnp.int32, (NU * SLP, CH), 0)
    wide_c = lax.broadcasted_iota(jnp.int32, (NU * SLP, CH), 1)
    spread = ((wide_r & 7) < SL) & (wide_c == (wide_r >> 3) * SL + (wide_r & 7))
    spread = spread.astype(F32).astype(BF)
    pack_r = lax.broadcasted_iota(jnp.int32, (CH, NU * SLP), 0)
    pack_c = lax.broadcasted_iota(jnp.int32, (CH, NU * SLP), 1)
    pack = ((pack_c & 7) < SL) & (pack_r == (pack_c >> 3) * SL + (pack_c & 7))
    pack = pack.astype(F32).astype(BF)

    def disp_copy(k):
        target = lax.rem(z + shift_of(k), NZ)
        return remote(
            disp.at[k], xin.at[k, y], zd_s.at[0], zd_r.at[k], at_zu(target, u), y
        )

    def rows_along(k, later):
        zz = lax.rem(z + shift_of(k), NZ)

        @pl.when(later < NZ)
        def _():
            send_rows(later, 0)

        landed = xdr.at[zz, pl.ds(0, NU - 1)]
        remote(landed, landed, xd_s.at[0], xd_r.at[k], ep, yp).wait_recv()
        xdr[zz, u] = xd[zz, u]

        def narrow(b, _):
            columns = pl.ds(pl.multiple_of(b * wide, wide), wide)
            rows = xdr[zz, :, :, columns].astype(F32).reshape(NU * SLP, wide).astype(BF)
            disp[k, :, columns] = dot(pack, rows).astype(BF)
            return 0

        lax.fori_loop(0, width // wide, narrow, 0, unroll=True)

        @pl.when(k != LOCAL)
        def _():
            disp_copy(k).start()

        @pl.when(k == LOCAL)
        def _():
            xin[k, y] = disp[k]

    def ag_copy(k, n, slot, columns, to):
        where = xin.at[k, slot, :, columns]
        return remote(where, where, ag_s.at[0], ag_r.at[k, n], ep, to)

    def ag_sends(k):
        return [
            ag_copy(k, 0, y, every, yp),
            ag_copy(k, 1, y, every, ym),
            ag_copy(k, 2, ym, low, yp),
            ag_copy(k, 3, yp, high, ym),
        ]

    def rows_out(k):
        @pl.when(k != LOCAL)
        def _():
            disp_copy(k).wait_recv()

        sends = ag_sends(k)
        sends[0].start()
        sends[1].start()

    rows_along(jnp.int32(1), jnp.int32(3))
    rows_along(jnp.int32(0), jnp.int32(4))
    rows_out(jnp.int32(0))
    rows_along(jnp.int32(2), jnp.int32(5))
    rows_along(jnp.int32(3), jnp.int32(6))
    for load in loads[7:]:
        load.wait()

    def rs_sends(k):
        return [
            remote(part.at[k, yo, :, low], rsa.at[k, 0], rs_s.at[0], rs_r.at[k, 0], ep, yp),
            remote(part.at[k, yo, :, high], rsa.at[k, 1], rs_s.at[0], rs_r.at[k, 1], ep, ym),
            remote(part.at[k, yp], rsb.at[k, 0], rs_s.at[0], rs_r.at[k, 2], ep, yp),
            remote(part.at[k, ym], rsb.at[k, 1], rs_s.at[0], rs_r.at[k, 3], ep, ym),
        ]

    def ret_copy(k, h):
        source = lax.rem(z - shift_of(k) + NZ, NZ)
        columns = (low, high)[h]
        return remote(
            ret.at[k, :, columns],
            back.at[k, :, columns],
            zr_s.at[0],
            zr_r.at[k, h],
            at_zu(source, u),
            y,
        )

    def xr_copy(k, d, columns):
        zz = lax.rem(z + shift_of(k), NZ)
        v = lax.rem(u + d, NU)
        return remote(
            xs.at[k, v, :, columns],
            xr.at[zz, u, :, columns],
            xr_s.at[0],
            xr_r.at[k],
            at_zu(z, v),
            y,
        )

    def rows_on(k):
        sends = ag_sends(k)
        ag_copy(k, 0, ym, every, yp).wait_recv()
        sends[2].start()
        ag_copy(k, 1, yp, every, ym).wait_recv()
        sends[3].start()

    def experts(k):
        ag_copy(k, 2, yo, low, yp).wait_recv()
        ag_copy(k, 3, yo, high, ym).wait_recv()
        rows = xin[k].reshape(NY * CH, width)
        ff = gate.shape[1]
        for b in range(ff // 256):
            columns = slice(b * 256, (b + 1) * 256)
            hid[:, columns] = (silu(dot(rows, gate[:, columns])) * dot(rows, up[:, columns])).astype(BF)

        def project(b, _):
            columns = pl.ds(pl.multiple_of(b * wide, wide), wide)
            out = dot(hid[...], down[:, columns]).astype(BF)
            part[k, :, :, columns] = out.reshape(NY, CH, wide)
            return 0

        lax.fori_loop(0, width // wide, project, 0)
        sends = rs_sends(k)
        sends[0].start()
        sends[1].start()

    def parts_on(k):
        sends = rs_sends(k)
        sends[0].wait_recv()
        kept = part[k, yp, :, low].astype(F32) + rsa[k, 0].astype(F32)
        part[k, yp, :, low] = kept.astype(BF)
        sends[2].start()
        sends[1].wait_recv()
        kept = part[k, ym, :, high].astype(F32) + rsa[k, 1].astype(F32)
        part[k, ym, :, high] = kept.astype(BF)
        sends[3].start()

    def results(k):
        sends = rs_sends(k)
        sends[2].wait_recv()
        sends[3].wait_recv()
        for h, columns in enumerate((low, high)):
            total = part[k, y, :, columns].astype(F32) + rsb[k, 0, :, columns].astype(F32)
            total = (total + rsb[k, 1, :, columns].astype(F32)).astype(BF)

            @pl.when(k != LOCAL)
            def _():
                ret[k, :, columns] = total
                ret_copy(k, h).start()

            @pl.when(k == LOCAL)
            def _():
                back[k, :, columns] = total

    def results_home(k):
        for h, columns in enumerate((low, high)):

            @pl.when(k != LOCAL)
            def _():
                ret_copy(k, h).wait_recv()

            for b in range(half // wide):
                some = pl.ds(h * half + b * wide, wide)
                out = dot(spread, back[k, :, some])
                xs[k, :, :, some] = out.reshape(NU, SLP, wide).astype(BF)

            def send(d, _):
                xr_copy(k, d, columns).start()
                return 0

            lax.fori_loop(1, NU, send, 0)
        xr[lax.rem(z + shift_of(k), NZ), u] = xs[k, u]

    def beside():
        rows = own[...]
        hidden = (silu(dot(rows, sgate[...])) * dot(rows, sup[...])).astype(BF)
        shared[...] = dot(hidden, sdown[...])
        for n, slot in enumerate((ym, yp)):
            conv_copy(n, slot, every, yp).wait_recv()
            conv_copy(n + 4, slot, every, yp).wait_recv()

        def project(n, _):
            conv_project(lax.rem(y + NY - 1 + n, NY))
            return 0

        lax.fori_loop(0, 3, project, 0)

    def conv_project(b):
        rows = pl.ds(pl.multiple_of(b * tokens, tokens), tokens)
        conv_out[rows, :] = dot(normed[b], ow[...]).astype(BF)

    def conv_forward():
        for n in (2, 3, 6, 7):
            conv_sends[n].start()

    def conv_last():
        for n in (2, 6):
            conv_copy(n, yo, low, yp).wait_recv()
            conv_copy(n + 1, yo, high, ym).wait_recv()
        conv_project(yo)

    def stage(i, lag, act):
        k = i - lag

        @pl.when((k >= 0) & (k < NZ))
        def _():
            act(k)

    def step(i, _):
        @pl.when((i >= 1) & (i < NZ))
        def _():
            rows_out(i)

        stage(i, 1, rows_on)

        stage(i, 2, experts)
        stage(i, 3, parts_on)

        @pl.when(i == NZ + 2)
        def _():
            conv_forward()

        stage(i, -EARLY, lambda k: rows_along(k, k + PACE))
        stage(i, 4, results)
        stage(i, HOME, results_home)

        @pl.when(i == 4)
        def _():
            beside()

        return 0

    lax.fori_loop(0, NZ + HOME, step, 0)
    conv_last()

    def arrived(k, _):
        landed = xr.at[lax.rem(z + shift_of(k), NZ), pl.ds(0, NU - 1)]
        remote(landed, landed, xr_s.at[0], xr_r.at[k], ep, yp).wait_recv()
        return 0

    lax.fori_loop(0, NZ, arrived, 0)

    def combine(b, _):
        columns = pl.ds(pl.multiple_of(b * wide, wide), wide)
        rows = xr[:, :, :, columns].astype(F32).reshape(NZ * NU * SLP, wide).astype(BF)
        both = dot(pick[...], rows)
        routed = both[0:tokens] * weights[:, 0:1] + both[tokens : 2 * tokens] * weights[:, 1:2]
        moe_out[:, columns] = (shared[:, columns] + routed).astype(BF)
        return 0

    lax.fori_loop(0, width // wide, combine, 0, unroll=2)

    halo_copy.wait_send()
    sent = pl.ds(0, NU - 1)
    for left, semaphore in (
        (normed.at[pl.ds(0, 3)], cv_s),
        (xd.at[sent], xd_s),
        (disp.at[sent], zd_s),
        (xin.at[:, pl.ds(0, 3)], ag_s),
        (part.at[:, pl.ds(0, 3)], rs_s),
        (ret.at[sent], zr_s),
        (xs.at[sent], xr_s),
    ):
        remote(left, left, semaphore.at[0], halo_sem.at[1], ep, yp).wait_send()


def on_device(*args):
    (
        conv_input,
        conv_kernel,
        conv_gain,
        out_weight,
        moe_input,
        moe_gain,
        expert_gate,
        expert_up,
        expert_down,
        shared_gate,
        shared_up,
        shared_down,
        expert_index,
        routing_weight,
    ) = args
    tokens, width = moe_input.shape
    half = width // 2
    ff = expert_gate.shape[2]
    cols = out_weight.shape[1]
    vm = lambda *shape, dtype=BF: pltpu.VMEM(shape, dtype)
    dma = lambda *shape: pltpu.SemaphoreType.DMA(shape)
    in_hbm = pl.BlockSpec(memory_space=pl.ANY)
    operands = (
        (conv_input, in_hbm),
        (conv_kernel, in_hbm),
        (conv_gain.reshape(1, width), in_hbm),
        (out_weight, in_hbm),
        (moe_input, in_hbm),
        (moe_gain.reshape(1, width), in_hbm),
        (expert_gate, in_hbm),
        (expert_up, in_hbm),
        (expert_down, in_hbm),
        (shared_gate, in_hbm),
        (shared_up, in_hbm),
        (shared_down, in_hbm),
        (expert_index.T, in_hbm),
        (routing_weight.T, in_hbm),
    )
    scratch = [
        vm(tokens, width),
        vm(*conv_kernel.shape, dtype=F32),
        vm(1, width, dtype=F32),
        vm(tokens, width),
        vm(1, width, dtype=F32),
        vm(*expert_index.shape[::-1], dtype=jnp.int32),
        vm(*routing_weight.shape[::-1], dtype=F32),
        vm(width, cols),
        vm(width, ff),
        vm(width, ff),
        vm(ff, width),
        vm(*shared_gate.shape),
        vm(*shared_up.shape),
        vm(*shared_down.shape),
        vm(EDGE, width),
        vm(width // 128, EDGE + tokens, 128, dtype=F32),
        vm(tokens, width, dtype=F32),
        vm(NY, tokens, width),
        vm(tokens, width),
        vm(NZ, NU * SLP, tokens),
        vm(NZ, NU, SLP, width),
        vm(NZ, NU, SLP, width),
        vm(NZ, CH, width),
        vm(NZ, NY, CH, width),
        vm(NY * CH, ff),
        vm(NZ, NY, CH, width),
        vm(NZ, 2, CH, half),
        vm(NZ, 2, CH, width),
        vm(NZ, CH, width),
        vm(NZ, CH, width),
        vm(NZ, NU, SLP, width),
        vm(NZ, NU, SLP, width),
        vm(2 * tokens, NZ * NU * SLP),
        vm(tokens, width, dtype=F32),
        vm(tokens, 128, dtype=F32),
        dma(14),
        dma(2),
        dma(1),
        dma(NZ),
        dma(1),
        dma(8),
        dma(1),
        dma(NZ),
        dma(1),
        dma(NZ, 4),
        dma(1),
        dma(NZ, 4),
        dma(1),
        dma(NZ, 2),
        dma(1),
        dma(NZ),
    ]
    shapes = (
        jax.ShapeDtypeStruct((NY * tokens, cols), BF),
        jax.ShapeDtypeStruct((tokens, width), BF),
    )
    in_vmem = pl.BlockSpec(memory_space=pltpu.VMEM)
    return pl.pallas_call(
        body,
        out_shape=tuple(pltpu.VMEM(shape.shape, BF) for shape in shapes),
        in_specs=[spec for _, spec in operands],
        out_specs=(in_vmem, in_vmem),
        scratch_shapes=scratch,
        compiler_params=pltpu.CompilerParams(
            collective_id=0, has_side_effects=True, vmem_limit_bytes=56 * 2**20
        ),
    )(*[array for array, _ in operands])

def solution(mesh):
    in_specs = (
        P(("ep", "tp"), None),
        P(),
        P(),
        P(None, "tp"),
        P(("ep", "tp"), None),
        P(),
        P("ep", None, "tp"),
        P("ep", None, "tp"),
        P("ep", "tp", None),
        P(),
        P(),
        P(),
        P("ep", None),
        P(("ep", "tp"), None),
    )
    out_specs = (P("ep", "tp"), P(("ep", "tp"), None))
    return jax.shard_map(
        on_device, mesh=mesh, in_specs=in_specs, out_specs=out_specs, check_vma=False
    )
```
